32 devices in a mesh: ep: 16 (over z, x, core), tp: 2 (over y).
Axes of the slice: x: 2, y: 2, z: 4, core: 2. Of those that a mesh axis runs over, the one named last changes fastest.
Arguments:
- tokens: bfloat16 [2048, 2048], P('ep'), may hold values from -6 to 6
- cotangent: bfloat16 [2048, 2048], P('ep'), may hold values from -1.796875 to 1.796875
- group_weight: float32 [2048], P('ep'), may hold values from 0.2 to 1
- expert_weight: float32 [2048, 2], P('ep'), may hold values from 0.1 to 0.9
- group_choice: int32 [2048], P('ep'), may hold values from 0 to 3, as said below
- local_choice: int32 [2048, 2], P('ep'), may hold values from 0 to 3, as said below
- w_gate: bfloat16 [16, 2048, 512], P('ep', None, 'tp'), may hold values from -0.125 to 0.125
- w_up: bfloat16 [16, 2048, 512], P('ep', None, 'tp'), may hold values from -0.125 to 0.125
- w_down: bfloat16 [16, 512, 2048], P('ep', 'tp'), may hold values from -0.25 to 0.25
Outputs:
- token_grad: float32 [2048, 2048], P('ep', 'tp')
- group_weight_grad: float32 [2048], P('ep')
- expert_weight_grad: float32 [2048, 2], P('ep')
- w_gate_grad: float32 [16, 2048, 512], P('ep', None, 'tp')
- w_up_grad: float32 [16, 2048, 512], P('ep', None, 'tp')
- w_down_grad: float32 [16, 512, 2048], P('ep', 'tp')
The draws below stay inside these ranges and needn't reach their ends.
Inputs may be any that keep to these rules, and one draw needn't show every extreme that they name: Among the 128 tokens of each device (aligned blocks of tokens), no expert 4 * group_choice + local_choice is named by more than 24 slots, and some expert is named by exactly 24 slots of every device. `local_choice`: the 2 local choices of a token differ.
All inputs are finite; a program needn't handle non-finite values.
Results may differ from the reference program's by a relative error of at most 0.006.
Values may be sent and summed in bfloat16 or wider, within the bound.
No kernel may reach another device: no remote copies, remote signals or barrier semaphores. Data moves between devices by JAX's collectives and lax.ppermute only.
A program may use at most 64 MiB of HBM per device.

```python
import math
import jax
import jax.numpy as jnp
from jax import lax

D = 2048
F = 512
EPG = 4
TOP_K = 2
TOK_DEV = 128
TOKENS = 2048
EXPERTS = 16
GROUPS = 4
CAP = 24
N_EP = 16


def route_tables(key):
    folded = jax.random.fold_in(key, 11)
    key_hot, key_perm, key_order, key_shift, key_step = jax.random.split(folded, 5)
    block_count = TOKENS // TOK_DEV
    busiest = EPG * CAP // TOP_K
    hot_group = jax.random.randint(key_hot, (), 0, GROUPS, dtype=jnp.int32)
    arrange = jax.vmap(lambda member_key: jax.random.permutation(member_key, TOK_DEV))(jax.random.split(key_perm, block_count)).astype(jnp.int32)
    others = jax.vmap(lambda member_key: jax.random.permutation(member_key, GROUPS - 1))(jax.random.split(key_order, block_count)).astype(jnp.int32)
    places = jnp.arange(TOK_DEV, dtype=jnp.int32)
    beyond = jnp.maximum(places - busiest, 0)
    column_ids = jnp.broadcast_to(beyond % (GROUPS - 1), (block_count, TOK_DEV))
    other_pick = jnp.take_along_axis(others, column_ids, axis=1)
    other_group = other_pick + (other_pick >= hot_group).astype(jnp.int32)
    group_at = jnp.where(places[None, :] < busiest, hot_group, other_group)
    rank_at = jnp.where(places < busiest, places, beyond // (GROUPS - 1))[None, :]
    shifts = jax.random.randint(key_shift, (block_count, GROUPS), 0, EPG, dtype=jnp.int32)
    strides = jax.random.randint(key_step, (block_count, GROUPS), 1, EPG, dtype=jnp.int32)
    first_local = (rank_at + jnp.take_along_axis(shifts, group_at, axis=1)) % EPG
    stride_at = jnp.take_along_axis(strides, group_at, axis=1)
    local_at = (first_local[..., None] + jnp.arange(TOP_K, dtype=jnp.int32) * stride_at[..., None]) % EPG
    inverse = jnp.argsort(arrange, axis=1, stable=True).astype(jnp.int32)
    group_table = jnp.take_along_axis(group_at, inverse, axis=1)
    local_table = jnp.take_along_axis(local_at, inverse[..., None], axis=1)
    return (group_table.reshape(TOKENS).astype(jnp.int32), local_table.reshape(TOKENS, TOP_K).astype(jnp.int32))


def draw_group_choice(key, part):
    return route_tables(key)[0]


def draw_local_choice(key, part):
    return route_tables(key)[1]


def level_of(own_key, extent, cuts, smallest, high):
    level = 1.0
    for dim, shards_of in cuts:
        draws = jax.random.uniform(jax.random.fold_in(jax.random.fold_in(own_key, 6), dim), (shards_of,), jnp.float32, smallest / len(cuts), high / len(cuts))
        level = level * jnp.repeat(jnp.exp(draws), extent[dim] // shards_of).reshape((-1,) + (1,) * (len(extent) - 1 - dim))
    return level


def noise(own_key, dims, scale, bound, cuts=(), kind=jnp.bfloat16):
    values = jax.random.normal(own_key, dims, jnp.float32) * scale
    if len(cuts) > 0:
        values = level_of(own_key, dims, cuts, -0.22, 0.18) * values
    return jnp.clip(values, min=-bound, max=bound).astype(kind)


def setup_inputs(seed: int = 0) -> dict:
    keys = jax.random.split(jax.random.key(seed), 10)
    return {
        "tokens": noise(keys[0], (TOKENS, D), 1.0, 6.0, ((0, 16),)),
        "cotangent": noise(keys[1], (TOKENS, D), 0.3, 1.796875, ((0, 16),)),
        "group_weight": jnp.clip(jnp.exp(math.log(1.0) - 1.609438 * jax.random.uniform(keys[2], (TOKENS,), jnp.float32) ** level_of(keys[2], (TOKENS,), ((0, 16),), -0.2, 0.2)), 0.2, 1.0),
        "expert_weight": jnp.clip(0.1 + 0.79999997 * jax.random.uniform(keys[3], (TOKENS, TOP_K), jnp.float32) ** level_of(keys[3], (TOKENS, TOP_K), ((0, 16),), -0.2, 0.2), 0.1, 0.9),
        "group_choice": draw_group_choice(jax.random.fold_in(keys[9], 71), 0),
        "local_choice": draw_local_choice(jax.random.fold_in(keys[9], 71), 0),
        "w_gate": noise(keys[6], (EXPERTS, D, F), D ** -0.5, 0.125, ((0, 16), (2, 2))),
        "w_up": noise(keys[7], (EXPERTS, D, F), D ** -0.5, 0.125, ((0, 16), (2, 2))),
        "w_down": noise(keys[8], (EXPERTS, F, D), F ** -0.5, 0.25, ((0, 16), (1, 2))),
    }


def expert_backward(arrived, cot_rows, gate_rows, first, second, third):
    pre_gate = jnp.dot(arrived, first, preferred_element_type=jnp.float32)
    pre_up = jnp.dot(arrived, second, preferred_element_type=jnp.float32)
    back_hidden = jnp.dot(cot_rows, third.T, preferred_element_type=jnp.float32)
    sigma = jax.nn.sigmoid(pre_gate)
    swish = pre_gate * sigma
    hidden = swish * pre_up
    gate_part = jnp.sum(hidden * back_hidden, axis=1)
    gate_float = gate_rows.astype(jnp.float32)[:, None]
    scaled = gate_float * back_hidden
    grad_gate_pre = (scaled * pre_up * sigma * (1.0 + pre_gate * (1.0 - sigma))).astype(jnp.bfloat16)
    grad_up_pre = (scaled * swish).astype(jnp.bfloat16)
    weighted = (gate_float * hidden).astype(jnp.bfloat16)
    first_grad = jnp.dot(arrived.T, grad_gate_pre, preferred_element_type=jnp.float32)
    second_grad = jnp.dot(arrived.T, grad_up_pre, preferred_element_type=jnp.float32)
    third_grad = jnp.dot(weighted.T, cot_rows, preferred_element_type=jnp.float32)
    total = jnp.dot(grad_gate_pre, first.T, preferred_element_type=jnp.float32)
    total = total + jnp.dot(grad_up_pre, second.T, preferred_element_type=jnp.float32)
    row_grad = total.astype(jnp.bfloat16)
    return first_grad, second_grad, third_grad, row_grad, gate_part


def reference(tokens, cotangent, group_weight, expert_weight, group_choice, local_choice, w_gate, w_up, w_down):
    slot_total = TOKENS * TOP_K
    expert_of = (group_choice[:, None] * EPG + local_choice).reshape(slot_total).astype(jnp.int32)
    member = (expert_of[:, None] == jnp.arange(EXPERTS, dtype=jnp.int32)[None, :]).astype(jnp.int32)
    running = jnp.cumsum(member, axis=0).astype(jnp.int32) - 1
    position = jnp.sum(running * member, axis=1).astype(jnp.int32)
    buffer_rows = N_EP * CAP
    slot_ids = jnp.arange(slot_total, dtype=jnp.int32)
    owner = jnp.full((EXPERTS, buffer_rows), slot_total, jnp.int32).at[expert_of, position].set(slot_ids)
    gate_value = (group_weight[:, None] * expert_weight).astype(jnp.bfloat16).reshape(slot_total)

    def per_expert(index):
        chosen = owner[index]
        live = chosen < slot_total
        safe = jnp.minimum(chosen, slot_total - 1)
        token_ids = (safe // TOP_K).astype(jnp.int32)
        zero = jnp.zeros((), jnp.bfloat16)
        arrived = jnp.where(live[:, None], tokens[token_ids], zero)
        cot_rows = jnp.where(live[:, None], cotangent[token_ids], zero)
        gate_rows = jnp.where(live, gate_value[safe], zero)
        return expert_backward(arrived, cot_rows, gate_rows, w_gate[index], w_up[index], w_down[index])

    first_grad, second_grad, third_grad, row_grad, gate_part = lax.map(per_expert, jnp.arange(EXPERTS, dtype=jnp.int32))
    slot_grad = row_grad[expert_of, position].astype(jnp.float32)
    token_grad = jnp.sum(slot_grad.reshape(TOKENS, TOP_K, D), axis=1)
    held = lax.optimization_barrier(gate_part[expert_of, position].astype(jnp.bfloat16))
    gate_grad = held.astype(jnp.float32).reshape(TOKENS, TOP_K)
    group_grad = jnp.sum(expert_weight * gate_grad, axis=1)
    expert_grad = group_weight[:, None] * gate_grad
    return (token_grad, group_grad, expert_grad, first_grad, second_grad, third_grad)
```

```python
import functools

import jax
import jax.numpy as jnp
from jax import lax
from jax.experimental import pallas as pl
from jax.experimental.pallas import tpu as pltpu
from jax.sharding import PartitionSpec as P

EPG = 4
LANES = 128
F32 = jnp.float32
BF16 = jnp.bfloat16

ROWS_COLS = (((1,), (1,)), ((), ()))
COLS_ROWS = (((1,), (0,)), ((), ()))
ROWS_ROWS = (((0,), (0,)), ((), ()))


def dot(a, b, dims):
    return lax.dot_general(a, b, dims, preferred_element_type=F32)


def vmem(count):
    return [pl.BlockSpec(memory_space=pltpu.VMEM)] * count


def call(body, outs, name, flops=0):
    def run(*args):
        return pl.pallas_call(
            body,
            out_shape=outs,
            in_specs=vmem(len(args)),
            out_specs=jax.tree.map(lambda _: pl.BlockSpec(memory_space=pltpu.VMEM), outs),
            compiler_params=pltpu.CompilerParams(vmem_limit_bytes=40 * 2**20),
            cost_estimate=pl.CostEstimate(flops=flops, bytes_accessed=0, transcendentals=0),
            name=name,
        )(*args)

    return run


def as_row(column):
    count = column.shape[0]
    eye = lax.broadcasted_iota(jnp.int32, (count, count), 0) == lax.broadcasted_iota(
        jnp.int32, (count, count), 1
    )
    return jnp.sum(jnp.where(eye, column, jnp.zeros_like(column)), axis=0, keepdims=True)


def route_body(groups, cap, width, *refs):
    choice_ref, local_ref, weight_ref, expert_ref, tok_ref, cot_ref = refs[:6]
    tok_out = refs[6 : 6 + groups]
    cot_out = refs[6 + groups : 6 + 2 * groups]
    pick_out = refs[6 + 2 * groups]
    count = tok_ref.shape[0]
    own = lax.axis_index("ep") // EPG
    start = pl.multiple_of(lax.axis_index("tp") * width, width)
    choice = choice_ref[...]
    padded = -(-groups // 8) * 8
    member = lax.broadcasted_iota(jnp.int32, (padded, count), 0) == choice
    before = (
        lax.broadcasted_iota(jnp.int32, (count, count), 0)
        < lax.broadcasted_iota(jnp.int32, (count, count), 1)
    ).astype(BF16)
    member = member.astype(F32)
    ahead = dot(member.astype(BF16), before, COLS_ROWS)
    place = jnp.sum(ahead * member, axis=0, keepdims=True).astype(jnp.int32)
    lane = lax.broadcasted_iota(jnp.int32, (LANES, count), 0)
    gates = jnp.zeros((LANES, count), F32)
    for k in range(local_ref.shape[1]):
        gate = (weight_ref[...] * as_row(expert_ref[:, k : k + 1])).astype(BF16).astype(F32)
        gates = gates + jnp.where(lane == as_row(local_ref[:, k : k + 1]), gate, 0.0)
    gates = gates.astype(BF16)
    tok = tok_ref[:, pl.ds(start, width)]
    cot = cot_ref[:, pl.ds(start, width)]
    slot = lax.broadcasted_iota(jnp.int32, (cap, count), 0)
    for k in range(groups):
        target = (own + k) % groups
        pick = ((slot == place) & (choice == target)).astype(F32).astype(BF16)
        pick_out[pl.ds(k * cap, cap), :] = pick
        tok_out[k][:, :width] = dot(pick, tok, COLS_ROWS).astype(BF16)
        tok_out[k][:, width:] = dot(pick, gates, ROWS_COLS).astype(BF16)
        cot_out[k][...] = dot(pick, cot, COLS_ROWS).astype(BF16)


def expert_body(lanes, width, *refs):
    tok = [refs[c * lanes : (c + 1) * lanes] for c in range(2)]
    cot = [refs[(2 + c) * lanes : (3 + c) * lanes] for c in range(2)]
    gate_w, up_w, down_w = refs[4 * lanes : 4 * lanes + 3]
    sums = refs[4 * lanes + 3 : 4 * lanes + 5]
    grads = refs[4 * lanes + 5 : 4 * lanes + 7]
    scaled_hidden = refs[4 * lanes + 7 : 4 * lanes + 9]
    rows = tok[0][0].shape[0]
    cols = gate_w.shape[1]
    mine = lax.axis_index("ep") % EPG
    rank = lax.axis_index("tp")
    spans = [
        pl.ds(pl.multiple_of(((rank + lanes - j) % lanes) * width, width), width)
        for j in range(lanes)
    ]
    lane = lax.broadcasted_iota(jnp.int32, (rows, LANES), 1)
    for c in range(2):
        pre_gate = jnp.zeros((rows, cols), F32)
        pre_up = jnp.zeros((rows, cols), F32)
        back = jnp.zeros((rows, cols), F32)
        for j in range(lanes):
            part = tok[c][j][:, :width]
            pre_gate = pre_gate + dot(part, gate_w[spans[j], :], COLS_ROWS)
            pre_up = pre_up + dot(part, up_w[spans[j], :], COLS_ROWS)
            back = back + dot(cot[c][j][...], down_w[:, spans[j]], ROWS_COLS)
        gates = tok[c][0][:, width:].astype(F32)
        gate = jnp.sum(jnp.where(lane == mine, gates, 0.0), axis=1, keepdims=True)
        sigma = jax.nn.sigmoid(pre_gate)
        swish = pre_gate * sigma
        hidden = swish * pre_up
        gate_part = jnp.sum(hidden * back, axis=1, keepdims=True)
        scaled = gate * back
        grad_gate = (scaled * pre_up * sigma * (1.0 + pre_gate * (1.0 - sigma))).astype(BF16)
        grad_up = (scaled * swish).astype(BF16)
        grads[c][:, :cols] = grad_gate
        grads[c][:, cols:] = grad_up
        scaled_hidden[c][...] = (gate * hidden).astype(BF16)
        for j in range(lanes):
            total = dot(grad_gate, gate_w[spans[j], :], ROWS_COLS)
            total = total + dot(grad_up, up_w[spans[j], :], ROWS_COLS)
            sums[c][:, j * width : (j + 1) * width] = total.astype(sums[c].dtype)
        high = gate_part.astype(BF16).astype(F32)
        low = gate_part - high
        tail = jnp.where(lane == mine, high, jnp.where(lane == mine + EPG, low, 0.0))
        sums[c][:, lanes * width :] = tail.astype(sums[c].dtype)


def weight_body(lanes, width, *refs):
    tok = [refs[b * lanes : (b + 1) * lanes] for b in range(4)]
    cot = [refs[(4 + b) * lanes : (5 + b) * lanes] for b in range(4)]
    grads = refs[8 * lanes : 8 * lanes + 4]
    scaled_hidden = refs[8 * lanes + 4 : 8 * lanes + 8]
    gate_out, up_out, down_out = refs[8 * lanes + 8 :]
    cols = gate_out.shape[1]
    rank = lax.axis_index("tp")
    chunk = min(width, 512)
    for j in range(lanes):
        base = ((rank + lanes - j) % lanes) * width
        for s in range(0, width, chunk):
            span = pl.ds(pl.multiple_of(base + s, chunk), chunk)
            total = dot(tok[0][j][:, s : s + chunk], grads[0][...], ROWS_ROWS)
            down = dot(scaled_hidden[0][...], cot[0][j][:, s : s + chunk], ROWS_ROWS)
            for b in range(1, 4):
                total = total + dot(tok[b][j][:, s : s + chunk], grads[b][...], ROWS_ROWS)
                down = down + dot(scaled_hidden[b][...], cot[b][j][:, s : s + chunk], ROWS_ROWS)
            gate_out[span, :] = total[:, :cols]
            up_out[span, :] = total[:, cols:]
            down_out[:, span] = down


def final_body(groups, cap, *refs):
    back = refs[:groups]
    pick_ref, local_ref, weight_ref, expert_ref = refs[groups : groups + 4]
    tok_out, group_out, expert_out = refs[groups + 4 :]
    count, width = tok_out.shape
    total = jnp.zeros((count, width + LANES), F32)
    for k in range(groups):
        pick = pick_ref[pl.ds(k * cap, cap), :]
        total = total + dot(pick, back[k][...], ROWS_ROWS)
    tok_out[...] = total[:, :width]
    held = total[:, width:]
    lane = lax.broadcasted_iota(jnp.int32, (count, LANES), 1)
    group_sum = jnp.zeros((count, 1), F32)
    eye = lax.broadcasted_iota(jnp.int32, (count, count), 0) == lax.broadcasted_iota(
        jnp.int32, (count, count), 1
    )
    weight = jnp.sum(jnp.where(eye, weight_ref[...], 0.0), axis=1, keepdims=True)
    for k in range(local_ref.shape[1]):
        grad = jnp.sum(
            jnp.where(lane == local_ref[:, k : k + 1], held, 0.0), axis=1, keepdims=True
        )
        group_sum = group_sum + expert_ref[:, k : k + 1] * grad
        expert_out[:, k : k + 1] = weight * grad
    group_out[...] = as_row(group_sum)


def shards(
    tokens, cotangent, group_weight, expert_weight, group_choice, local_choice, w_gate, w_up, w_down
):
    count, features = tokens.shape
    picks = expert_weight.shape[1]
    experts = lax.axis_size("ep")
    lanes = lax.axis_size("tp")
    groups = experts // EPG
    width = features // lanes
    capacity = picks * (3 * count // (2 * experts))
    cap = min(count, EPG * capacity // picks)
    cap = -(-cap // 16) * 16
    rows = groups * cap
    cols = w_gate.shape[2]

    def along_groups(a, k):
        pairs = [(e, (e // EPG + k) % groups * EPG + e % EPG) for e in range(experts)]
        return lax.ppermute(a, "ep", pairs)

    def along_side(a):
        return lax.ppermute(a, "ep", [(e, e ^ 2) for e in range(experts)])

    def along_core(a):
        return lax.ppermute(a, "ep", [(e, e ^ 1) for e in range(experts)])

    def along_tp(a, j):
        return lax.ppermute(a, "tp", [(r, (r + j) % lanes) for r in range(lanes)])

    shape = jax.ShapeDtypeStruct
    choice_row = group_choice.reshape(1, count)
    weight_row = group_weight.reshape(1, count)
    routed = call(
        functools.partial(route_body, groups, cap, width),
        [shape((cap, width + LANES), BF16)] * groups
        + [shape((cap, width), BF16)] * groups
        + [shape((rows, count), BF16)],
        "route",
    )(choice_row, local_choice, weight_row, expert_weight, tokens, cotangent)
    picked = routed[2 * groups]
    tok_sent = [routed[0]] + [along_groups(routed[k], k) for k in range(1, groups)]
    cot_sent = [routed[groups]] + [along_groups(routed[groups + k], k) for k in range(1, groups)]
    tok = jnp.concatenate(tok_sent, axis=0)
    cot = jnp.concatenate(cot_sent, axis=0)
    tok_side = along_side(tok)
    tok_lane = [along_tp(tok, j) for j in range(1, lanes)]
    cot_side = along_side(cot)
    cot_lane = [along_tp(cot, j) for j in range(1, lanes)]
    tok_both = [along_tp(tok_side, j) for j in range(1, lanes)]
    cot_both = [along_side(a) for a in cot_lane]
    tok_near = [tok] + tok_lane
    cot_near = [cot] + cot_lane
    tok_far = [tok_side] + tok_both
    cot_far = [cot_side] + cot_both
    first, second, third = w_gate[0], w_up[0], w_down[0]
    work = 2 * 5 * 2 * rows * features * cols

    def experts_on(tok_list, cot_list, name):
        tok_other = [along_core(a) for a in tok_list]
        cot_other = [along_core(a) for a in cot_list]
        outs = call(
            functools.partial(expert_body, lanes, width),
            [shape((rows, features + LANES), F32), shape((rows, features + LANES), BF16)]
            + [shape((rows, 2 * cols), BF16)] * 2
            + [shape((rows, cols), BF16)] * 2,
            name,
            work,
        )(*tok_list, *tok_other, *cot_list, *cot_other, first, second, third)
        return outs, tok_list + tok_other, cot_list + cot_other

    near, tok_a, cot_a = experts_on(tok_near, cot_near, "near")
    far, tok_b, cot_b = experts_on(tok_far, cot_far, "far")
    near_sum = near[0] + along_core(near[1]).astype(F32)
    far_sum = far[0] + along_core(far[1]).astype(F32)
    if lanes == 2:
        half = width // 2
        tail = far_sum[:, features:]
        side_out = jnp.concatenate(
            [far_sum[:, :half], far_sum[:, width : width + half], tail], axis=1
        ).astype(BF16)
        lane_out = jnp.concatenate(
            [near_sum[:, width + half : features], far_sum[:, width + half : features]], axis=0
        ).astype(BF16)
        side_in = along_side(side_out).astype(F32)
        lane_in = along_tp(lane_out, 1).astype(F32)
        lane_next = jnp.concatenate(
            [
                near_sum[:, width : width + half] + side_in[:, half:width],
                near_sum[:, features:] + side_in[:, width:],
            ],
            axis=1,
        )
        side_next = (far_sum[:, half:width] + lane_in[rows:]).astype(BF16)
        lane_last = along_tp(lane_next.astype(BF16), 1).astype(F32)
        side_last = along_side(side_next).astype(F32)
        tail = lane_next[:, half:] + lane_last[:, half:]
        body = jnp.concatenate(
            [
                near_sum[:, :half] + side_in[:, :half] + lane_last[:, :half],
                near_sum[:, half:width] + lane_in[:rows] + side_last,
            ],
            axis=1,
        )
    else:
        both = near_sum + along_side(far_sum.astype(BF16)).astype(F32)
        tail = both[:, features:]
        body = both[:, :width]
        for j in range(1, lanes):
            piece = jnp.concatenate(
                [both[:, j * width : (j + 1) * width], both[:, features:]], axis=1
            )
            piece = along_tp(piece.astype(BF16), lanes - j).astype(F32)
            body = body + piece[:, :width]
            tail = tail + piece[:, width:]
    held = tail[:, :EPG] + tail[:, EPG : 2 * EPG]
    held = jnp.pad(held, ((0, 0), (0, LANES - EPG)))
    result = jnp.concatenate([body, held], axis=1).astype(BF16)
    returned = [result[:cap]] + [
        along_groups(result[k * cap : (k + 1) * cap], groups - k) for k in range(1, groups)
    ]
    grads = list(near[2:4]) + list(far[2:4])
    scaled_hidden = list(near[4:6]) + list(far[4:6])
    first_grad, second_grad, third_grad = call(
        functools.partial(weight_body, lanes, width),
        [shape((features, cols), F32)] * 2 + [shape((cols, features), F32)],
        "weights",
        2 * 3 * 4 * rows * features * cols,
    )(*tok_a, *tok_b, *cot_a, *cot_b, *grads, *scaled_hidden)
    token_grad, group_grad, expert_grad = call(
        functools.partial(final_body, groups, cap),
        [shape((count, width), F32), shape((1, count), F32), shape((count, picks), F32)],
        "final",
    )(*returned, picked, local_choice, weight_row, expert_weight)
    return (
        token_grad,
        group_grad.reshape(count),
        expert_grad,
        first_grad[None],
        second_grad[None],
        third_grad[None],
    )


def solution(mesh):
    in_specs = (
        P("ep", None),
        P("ep", None),
        P("ep"),
        P("ep", None),
        P("ep"),
        P("ep", None),
        P("ep", None, "tp"),
        P("ep", None, "tp"),
        P("ep", "tp", None),
    )
    out_specs = (
        P("ep", "tp"),
        P("ep"),
        P("ep", None),
        P("ep", None, "tp"),
        P("ep", None, "tp"),
        P("ep", "tp", None),
    )
    return jax.shard_map(shards, mesh=mesh, in_specs=in_specs, out_specs=out_specs, check_vma=False)
```

```python
import functools

import jax
import jax.numpy as jnp
from jax import lax
from jax.experimental import pallas as pl
from jax.experimental.pallas import tpu as pltpu
from jax.sharding import PartitionSpec as P


EPG = 4
LANES = 128
F32 = jnp.float32
BF16 = jnp.bfloat16

ROWS_COLS = (((1,), (1,)), ((), ()))
COLS_ROWS = (((1,), (0,)), ((), ()))
ROWS_ROWS = (((0,), (0,)), ((), ()))


def dot(a, b, dims):
    return lax.dot_general(a, b, dims, preferred_element_type=F32)


def call(body, outs, flops=0, space=pltpu.VMEM, scratch=()):
    def run(*args):
        return pl.pallas_call(
            body,
            out_shape=outs,
            in_specs=[pl.BlockSpec(memory_space=space)] * len(args),
            out_specs=jax.tree.map(lambda _: pl.BlockSpec(memory_space=pltpu.VMEM), outs),
            scratch_shapes=scratch,
            compiler_params=pltpu.CompilerParams(vmem_limit_bytes=40 * 2**20),
            cost_estimate=pl.CostEstimate(flops=flops, bytes_accessed=0, transcendentals=0),
        )(*args)

    return run


def route_body(groups, cap, width, *refs):
    sources = refs[:6]
    own_out = refs[6]
    tok_out = refs[7 : 6 + groups]
    cot_out = refs[6 + groups : 5 + 2 * groups]
    choice_ref, local_ref, weight_ref, expert_ref, tok_ref, cot_ref, sems = refs[5 + 2 * groups :]
    count = tok_ref.shape[0]
    own = lax.axis_index("ep") // EPG
    start = pl.multiple_of(lax.axis_index("tp") * width, width)
    copies = []
    for k, (src, dst) in enumerate(
        zip(sources, (choice_ref, local_ref, weight_ref, expert_ref, tok_ref, cot_ref))
    ):
        if k >= 4:
            src = src.at[:, pl.ds(start, width)]
        copies.append(pltpu.make_async_copy(src, dst, sems.at[k]))
    for copy in copies:
        copy.start()
    for copy in copies[:4]:
        copy.wait()
    choice = choice_ref[...]
    padded = -(-groups // 8) * 8
    member = lax.broadcasted_iota(jnp.int32, (padded, count), 0) == choice
    before = (
        lax.broadcasted_iota(jnp.int32, (count, count), 0)
        < lax.broadcasted_iota(jnp.int32, (count, count), 1)
    ).astype(BF16)
    member = member.astype(F32)
    ahead = dot(member.astype(BF16), before, COLS_ROWS)
    place = jnp.sum(ahead * member, axis=0, keepdims=True).astype(jnp.int32)
    lane = lax.broadcasted_iota(jnp.int32, (LANES, count), 0)
    gates = jnp.zeros((LANES, count), F32)
    for k in range(local_ref.shape[0]):
        gate = (weight_ref[...] * expert_ref[k : k + 1, :]).astype(BF16).astype(F32)
        gates = gates + jnp.where(lane == local_ref[k : k + 1, :], gate, 0.0)
    gates = gates.astype(BF16)
    slot = lax.broadcasted_iota(jnp.int32, (cap, count), 0)
    picks = [
        ((slot == place) & (choice == (own ^ k))).astype(F32).astype(BF16)
        for k in range(groups)
    ]
    gate_rows = [dot(pick, gates, ROWS_COLS).astype(BF16) for pick in picks]
    copies[4].wait()
    for k in range(1, groups):
        tok_out[k - 1][...] = dot(picks[k], tok_ref[...], COLS_ROWS).astype(BF16)
    own_out[:, :width] = dot(picks[0], tok_ref[...], COLS_ROWS).astype(BF16)
    copies[5].wait()
    for k in range(1, groups):
        cot_out[k - 1][:, :width] = dot(picks[k], cot_ref[...], COLS_ROWS).astype(BF16)
        cot_out[k - 1][:, width:] = gate_rows[k]
    own_out[:, width : 2 * width] = dot(picks[0], cot_ref[...], COLS_ROWS).astype(BF16)
    own_out[:, 2 * width :] = gate_rows[0]


def picks_body(groups, cap, parts, choice_ref, out_ref):
    choice = choice_ref[...]
    count = choice.shape[1]
    own = lax.axis_index("ep") // EPG
    padded = -(-groups // 8) * 8
    member = (lax.broadcasted_iota(jnp.int32, (padded, count), 0) == choice).astype(F32)
    before = (
        lax.broadcasted_iota(jnp.int32, (count, count), 0)
        < lax.broadcasted_iota(jnp.int32, (count, count), 1)
    ).astype(BF16)
    ahead = dot(member.astype(BF16), before, COLS_ROWS)
    place = jnp.sum(ahead * member, axis=0, keepdims=True).astype(jnp.int32)
    slot = lax.broadcasted_iota(jnp.int32, (cap, count), 0)
    for i, k in enumerate(parts):
        pick = (slot == place) & (choice == (own ^ k))
        out_ref[pl.ds(i * cap, cap), :] = pick.astype(F32).astype(BF16)


def expert_body(lanes, width, *refs):
    tok = [refs[c * lanes : (c + 1) * lanes] for c in range(2)]
    cot = [refs[(2 + c) * lanes : (3 + c) * lanes] for c in range(2)]
    gate_w, up_w, down_w = refs[4 * lanes : 4 * lanes + 3]
    sums = refs[4 * lanes + 3 : 4 * lanes + 5]
    grads = refs[4 * lanes + 5 : 4 * lanes + 7]
    scaled_hidden = refs[4 * lanes + 7 : 4 * lanes + 9]
    rows = tok[0][0].shape[0]
    cols = gate_w.shape[1]
    mine = lax.axis_index("ep") % EPG
    rank = lax.axis_index("tp")
    spans = [
        pl.ds(pl.multiple_of(((rank + lanes - j) % lanes) * width, width), width)
        for j in range(lanes)
    ]
    lane = lax.broadcasted_iota(jnp.int32, (rows, LANES), 1)
    for c in range(2):
        pre_gate = jnp.zeros((rows, cols), F32)
        pre_up = jnp.zeros((rows, cols), F32)
        back = jnp.zeros((rows, cols), F32)
        for j in range(lanes):
            part = tok[c][j][...]
            pre_gate = pre_gate + dot(part, gate_w[spans[j], :], COLS_ROWS)
            pre_up = pre_up + dot(part, up_w[spans[j], :], COLS_ROWS)
            back = back + dot(cot[c][j][:, :width], down_w[:, spans[j]], ROWS_COLS)
        gates = cot[c][0][:, width:].astype(F32)
        gate = jnp.sum(jnp.where(lane == mine, gates, 0.0), axis=1, keepdims=True)
        sigma = jax.nn.sigmoid(pre_gate)
        swish = pre_gate * sigma
        hidden = swish * pre_up
        gate_part = jnp.sum(hidden * back, axis=1, keepdims=True)
        scaled = gate * back
        grad_gate = (scaled * pre_up * sigma * (1.0 + pre_gate * (1.0 - sigma))).astype(BF16)
        grad_up = (scaled * swish).astype(BF16)
        grads[c][:, :cols] = grad_gate
        grads[c][:, cols:] = grad_up
        scaled_hidden[c][...] = (gate * hidden).astype(BF16)
        for j in range(lanes):
            total = dot(grad_gate, gate_w[spans[j], :], ROWS_COLS)
            total = total + dot(grad_up, up_w[spans[j], :], ROWS_COLS)
            sums[c][:, j * width : (j + 1) * width] = total.astype(sums[c].dtype)
        high = gate_part.astype(BF16).astype(F32)
        low = gate_part - high
        tail = jnp.where(lane == mine, high, jnp.where(lane == mine + EPG, low, 0.0))
        sums[c][:, lanes * width :] = tail.astype(sums[c].dtype)


def weight_body(lanes, width, *refs):
    tok = [refs[b * lanes : (b + 1) * lanes] for b in range(4)]
    cot = [refs[(4 + b) * lanes : (5 + b) * lanes] for b in range(4)]
    grads = refs[8 * lanes : 8 * lanes + 4]
    scaled_hidden = refs[8 * lanes + 4 : 8 * lanes + 8]
    gate_out, up_out, down_out = refs[8 * lanes + 8 :]
    cols = gate_out.shape[1]
    rank = lax.axis_index("tp")
    chunk = min(width, 512)
    for j in range(lanes):
        base = ((rank + lanes - j) % lanes) * width
        for s in range(0, width, chunk):
            span = pl.ds(pl.multiple_of(base + s, chunk), chunk)
            total = dot(tok[0][j][:, s : s + chunk], grads[0][...], ROWS_ROWS)
            down = dot(scaled_hidden[0][...], cot[0][j][:, s : s + chunk], ROWS_ROWS)
            for b in range(1, 4):
                total = total + dot(tok[b][j][:, s : s + chunk], grads[b][...], ROWS_ROWS)
                down = down + dot(scaled_hidden[b][...], cot[b][j][:, s : s + chunk], ROWS_ROWS)
            gate_out[span, :] = total[:, :cols]
            up_out[span, :] = total[:, cols:]
            down_out[:, span] = down


def final_body(groups, cap, *refs):
    back = refs[:groups]
    pick_refs = refs[groups : groups + 3]
    local_ref, weight_ref, expert_ref = refs[groups + 3 : groups + 6]
    tok_out, group_out, expert_out = refs[groups + 6 :]
    count, width = tok_out.shape
    total = jnp.zeros((count, width), F32)
    held = jnp.zeros((LANES, count), F32)
    for k in range(groups):
        pick = pick_refs[min(k, 2)][pl.ds(max(k - 2, 0) * cap, cap), :]
        total = total + dot(pick, back[k][:, :width], ROWS_ROWS)
        held = held + dot(back[k][:, width:], pick, ROWS_ROWS)
    tok_out[...] = total
    lane = lax.broadcasted_iota(jnp.int32, (LANES, count), 0)
    group_sum = jnp.zeros((1, count), F32)
    for k in range(local_ref.shape[0]):
        grad = jnp.sum(
            jnp.where(lane == local_ref[k : k + 1, :], held, 0.0), axis=0, keepdims=True
        )
        group_sum = group_sum + expert_ref[k : k + 1, :] * grad
        expert_out[k : k + 1, :] = weight_ref[...] * grad
    group_out[...] = group_sum


def layer(
    tokens, cotangent, group_weight, expert_weight, group_choice, local_choice, w_gate, w_up, w_down
):
    count, features = tokens.shape
    picks = expert_weight.shape[1]
    experts = lax.axis_size("ep")
    lanes = lax.axis_size("tp")
    groups = experts // EPG
    width = features // lanes
    capacity = picks * (3 * count // (2 * experts))
    cap = min(count, EPG * capacity // picks)
    cap = -(-cap // 16) * 16
    rows = groups * cap
    cols = w_gate.shape[2]

    def along_groups(a, k):
        return lax.ppermute(a, "ep", [(e, e ^ (k * EPG)) for e in range(experts)])

    def along_side(a):
        return lax.ppermute(a, "ep", [(e, e ^ 2) for e in range(experts)])

    def along_core(a):
        return lax.ppermute(a, "ep", [(e, e ^ 1) for e in range(experts)])

    def along_tp(a, j):
        return lax.ppermute(a, "tp", [(r, (r + j) % lanes) for r in range(lanes)])

    shape = jax.ShapeDtypeStruct
    choice_row = group_choice.reshape(1, count)
    weight_row = group_weight.reshape(1, count)
    local_rows = local_choice.T
    expert_rows = expert_weight.T
    routed = call(
        functools.partial(route_body, groups, cap, width),
        [shape((cap, 2 * width + LANES), BF16)]
        + [shape((cap, width), BF16)] * (groups - 1)
        + [shape((cap, width + LANES), BF16)] * (groups - 1),
        space=pltpu.HBM,
        scratch=[
            pltpu.VMEM((1, count), jnp.int32),
            pltpu.VMEM((picks, count), jnp.int32),
            pltpu.VMEM((1, count), F32),
            pltpu.VMEM((picks, count), F32),
            pltpu.VMEM((count, width), BF16),
            pltpu.VMEM((count, width), BF16),
            pltpu.SemaphoreType.DMA((6,)),
        ],
    )(
        *(
            pltpu.with_memory_space_constraint(a, pltpu.HBM)
            for a in (choice_row, local_rows, weight_row, expert_rows, tokens, cotangent)
        )
    )
    parts = [[0], [1], list(range(2, groups))]
    picked = [
        call(
            functools.partial(picks_body, groups, cap, part),
            shape((len(part) * cap, count), BF16),
            10**6,
        )(choice_row)
        for part in parts
    ]
    own = routed[0]
    others = range(groups - 1, 0, -1)
    tok_sent = {k: along_groups(routed[k], k) for k in others}
    own_side = along_side(own)
    own_lane = [along_tp(own, j) for j in range(1, lanes)]
    cot_sent = {k: along_groups(routed[groups - 1 + k], k) for k in others}
    own_tok_both = [along_tp(own_side[:, :width], j) for j in range(1, lanes)]
    own_cot_both = [along_side(a[:, width : 2 * width]) for a in own_lane]
    tok = jnp.concatenate([tok_sent[k] for k in range(1, groups)], axis=0)
    cot = jnp.concatenate([cot_sent[k] for k in range(1, groups)], axis=0)
    cot_bare = jnp.concatenate([cot_sent[k][:, :width] for k in range(1, groups)], axis=0)
    tok_side = along_side(tok)
    tok_lane = [along_tp(tok, j) for j in range(1, lanes)]
    cot_side = along_side(cot)
    cot_lane = [along_tp(cot_bare, j) for j in range(1, lanes)]
    cut = width // 2 if width % (2 * LANES) == 0 else width

    def diagonal(side, lane):
        parts_a = [along_tp(side[:, :cut], j) for j in range(1, lanes)]
        if cut == width:
            return parts_a
        parts_b = [along_side(a[:, cut:width]) for a in lane]
        return [jnp.concatenate([a, b], axis=1) for a, b in zip(parts_a, parts_b)]

    tok_both = diagonal(tok_side, tok_lane)
    cot_both = diagonal(cot_side, cot_lane)

    def join(head, rest):
        return jnp.concatenate([head, rest], axis=0)

    tok_near = [join(own[:, :width], tok)]
    tok_near += [join(a[:, :width], b) for a, b in zip(own_lane, tok_lane)]
    cot_near = [join(own[:, width:], cot)]
    cot_near += [join(a[:, width : 2 * width], b) for a, b in zip(own_lane, cot_lane)]
    tok_far = [join(own_side[:, :width], tok_side)]
    tok_far += [join(a, b) for a, b in zip(own_tok_both, tok_both)]
    cot_far = [join(own_side[:, width:], cot_side)]
    cot_far += [join(a, b) for a, b in zip(own_cot_both, cot_both)]
    first, second, third = w_gate[0], w_up[0], w_down[0]
    work = 2 * 5 * 2 * rows * features * cols

    def experts_on(tok_list, cot_list):
        tok_other = [along_core(a) for a in tok_list]
        cot_other = [along_core(a) for a in cot_list]
        outs = call(
            functools.partial(expert_body, lanes, width),
            [shape((rows, features + LANES), F32), shape((rows, features + LANES), BF16)]
            + [shape((rows, 2 * cols), BF16)] * 2
            + [shape((rows, cols), BF16)] * 2,
            work,
        )(*tok_list, *tok_other, *cot_list, *cot_other, first, second, third)
        return outs, tok_list + tok_other, cot_list + cot_other

    near, tok_a, cot_a = experts_on(tok_near, cot_near)
    far, tok_b, cot_b = experts_on(tok_far, cot_far)
    near_sum = near[0] + along_core(near[1]).astype(F32)
    far_sum = far[0] + along_core(far[1]).astype(F32)
    if lanes == 2:
        half = width // 2
        tail = far_sum[:, features:]
        side_out = jnp.concatenate(
            [far_sum[:, :half], far_sum[:, width : width + half], tail], axis=1
        ).astype(BF16)
        lane_out = jnp.concatenate(
            [near_sum[:, width + half : features], far_sum[:, width + half : features]], axis=0
        ).astype(BF16)
        side_in = along_side(side_out).astype(F32)
        lane_in = along_tp(lane_out, 1).astype(F32)
        lane_next = jnp.concatenate(
            [
                near_sum[:, width : width + half] + side_in[:, half:width],
                near_sum[:, features:] + side_in[:, width:],
            ],
            axis=1,
        )
        side_next = (far_sum[:, half:width] + lane_in[rows:]).astype(BF16)
        lane_last = along_tp(lane_next.astype(BF16), 1).astype(F32)
        side_last = along_side(side_next).astype(F32)
        tail = lane_next[:, half:] + lane_last[:, half:]
        body = jnp.concatenate(
            [
                near_sum[:, :half] + side_in[:, :half] + lane_last[:, :half],
                near_sum[:, half:width] + lane_in[:rows] + side_last,
            ],
            axis=1,
        )
    else:
        both = near_sum + along_side(far_sum.astype(BF16)).astype(F32)
        tail = both[:, features:]
        body = both[:, :width]
        for j in range(1, lanes):
            piece = jnp.concatenate(
                [both[:, j * width : (j + 1) * width], both[:, features:]], axis=1
            )
            piece = along_tp(piece.astype(BF16), lanes - j).astype(F32)
            body = body + piece[:, :width]
            tail = tail + piece[:, width:]
    held = tail[:, :EPG] + tail[:, EPG : 2 * EPG]
    held = jnp.pad(held, ((0, 0), (0, LANES - EPG)))
    result = jnp.concatenate([body, held], axis=1).astype(BF16)
    sent = {k: along_groups(result[k * cap : (k + 1) * cap], k) for k in others}
    returned = [result[:cap]] + [sent[k] for k in range(1, groups)]
    grads = list(near[2:4]) + list(far[2:4])
    scaled_hidden = list(near[4:6]) + list(far[4:6])
    first_grad, second_grad, third_grad = call(
        functools.partial(weight_body, lanes, width),
        [shape((features, cols), F32)] * 2 + [shape((cols, features), F32)],
        2 * 3 * 4 * rows * features * cols,
    )(*tok_a, *tok_b, *cot_a, *cot_b, *grads, *scaled_hidden)
    token_grad, group_grad, expert_grad = call(
        functools.partial(final_body, groups, cap),
        [shape((count, width), F32), shape((1, count), F32), shape((picks, count), F32)],
    )(*returned, *picked, local_rows, weight_row, expert_rows)
    return (
        token_grad,
        group_grad.reshape(count),
        expert_grad.T,
        first_grad[None],
        second_grad[None],
        third_grad[None],
    )


def solution(mesh):
    in_specs = (
        P("ep", None),
        P("ep", None),
        P("ep"),
        P("ep", None),
        P("ep"),
        P("ep", None),
        P("ep", None, "tp"),
        P("ep", None, "tp"),
        P("ep", "tp", None),
    )
    out_specs = (
        P("ep", "tp"),
        P("ep"),
        P("ep", None),
        P("ep", None, "tp"),
        P("ep", None, "tp"),
        P("ep", "tp", None),
    )
    return jax.shard_map(layer, mesh=mesh, in_specs=in_specs, out_specs=out_specs, check_vma=False)
```

```python
import functools

import jax
import jax.numpy as jnp
from jax import lax
from jax.experimental import pallas as pl
from jax.experimental.pallas import tpu as pltpu
from jax.sharding import PartitionSpec as P


EPG = 4
LANES = 128
F32 = jnp.float32
BF16 = jnp.bfloat16

ROWS_COLS = (((1,), (1,)), ((), ()))
COLS_ROWS = (((1,), (0,)), ((), ()))
ROWS_ROWS = (((0,), (0,)), ((), ()))


def dot(a, b, dims):
    return lax.dot_general(a, b, dims, preferred_element_type=F32)


def call(body, outs, flops=0, space=pltpu.VMEM, scratch=()):
    def run(*args):
        return pl.pallas_call(
            body,
            out_shape=outs,
            in_specs=[pl.BlockSpec(memory_space=space)] * len(args),
            out_specs=jax.tree.map(lambda _: pl.BlockSpec(memory_space=pltpu.VMEM), outs),
            scratch_shapes=scratch,
            compiler_params=pltpu.CompilerParams(vmem_limit_bytes=40 * 2**20),
            cost_estimate=pl.CostEstimate(flops=flops, bytes_accessed=0, transcendentals=0),
        )(*args)

    return run


def route_body(groups, cap, width, *refs):
    sources = refs[:6]
    own_out = refs[6]
    tok_out = refs[7 : 6 + groups]
    cot_out = refs[6 + groups : 5 + 2 * groups]
    choice_ref, local_ref, weight_ref, expert_ref, tok_ref, cot_ref, sems = refs[5 + 2 * groups :]
    count = tok_ref.shape[0]
    own = lax.axis_index("ep") // EPG
    start = pl.multiple_of(lax.axis_index("tp") * width, width)
    copies = []
    for k, (src, dst) in enumerate(
        zip(sources, (choice_ref, local_ref, weight_ref, expert_ref, tok_ref, cot_ref))
    ):
        if k >= 4:
            src = src.at[:, pl.ds(start, width)]
        copies.append(pltpu.make_async_copy(src, dst, sems.at[k]))
    for copy in copies:
        copy.start()
    for copy in copies[:4]:
        copy.wait()
    choice = choice_ref[...]
    padded = -(-groups // 8) * 8
    member = lax.broadcasted_iota(jnp.int32, (padded, count), 0) == choice
    before = (
        lax.broadcasted_iota(jnp.int32, (count, count), 0)
        < lax.broadcasted_iota(jnp.int32, (count, count), 1)
    ).astype(BF16)
    member = member.astype(F32)
    ahead = dot(member.astype(BF16), before, COLS_ROWS)
    place = jnp.sum(ahead * member, axis=0, keepdims=True).astype(jnp.int32)
    lane = lax.broadcasted_iota(jnp.int32, (LANES, count), 0)
    gates = jnp.zeros((LANES, count), F32)
    for k in range(local_ref.shape[0]):
        gate = (weight_ref[...] * expert_ref[k : k + 1, :]).astype(BF16).astype(F32)
        gates = gates + jnp.where(lane == local_ref[k : k + 1, :], gate, 0.0)
    gates = gates.astype(BF16)
    slot = lax.broadcasted_iota(jnp.int32, (cap, count), 0)
    picks = [
        ((slot == place) & (choice == (own ^ k))).astype(F32).astype(BF16)
        for k in range(groups)
    ]
    gate_rows = [dot(pick, gates, ROWS_COLS).astype(BF16) for pick in picks]
    copies[4].wait()
    for k in range(1, groups):
        tok_out[k - 1][...] = dot(picks[k], tok_ref[...], COLS_ROWS).astype(BF16)
    own_out[:, :width] = dot(picks[0], tok_ref[...], COLS_ROWS).astype(BF16)
    copies[5].wait()
    for k in range(1, groups):
        cot_out[k - 1][:, :width] = dot(picks[k], cot_ref[...], COLS_ROWS).astype(BF16)
        cot_out[k - 1][:, width:] = gate_rows[k]
    own_out[:, width : 2 * width] = dot(picks[0], cot_ref[...], COLS_ROWS).astype(BF16)
    own_out[:, 2 * width :] = gate_rows[0]


def picks_body(groups, cap, parts, choice_ref, out_ref):
    choice = choice_ref[...]
    count = choice.shape[1]
    own = lax.axis_index("ep") // EPG
    padded = -(-groups // 8) * 8
    member = (lax.broadcasted_iota(jnp.int32, (padded, count), 0) == choice).astype(F32)
    before = (
        lax.broadcasted_iota(jnp.int32, (count, count), 0)
        < lax.broadcasted_iota(jnp.int32, (count, count), 1)
    ).astype(BF16)
    ahead = dot(member.astype(BF16), before, COLS_ROWS)
    place = jnp.sum(ahead * member, axis=0, keepdims=True).astype(jnp.int32)
    slot = lax.broadcasted_iota(jnp.int32, (cap, count), 0)
    for i, k in enumerate(parts):
        pick = (slot == place) & (choice == (own ^ k))
        out_ref[pl.ds(i * cap, cap), :] = pick.astype(F32).astype(BF16)


def expert_body(lanes, width, *refs):
    tok = [refs[c * lanes : (c + 1) * lanes] for c in range(2)]
    cot = [refs[(2 + c) * lanes : (3 + c) * lanes] for c in range(2)]
    gate_w, up_w, down_w = refs[4 * lanes : 4 * lanes + 3]
    sums = refs[4 * lanes + 3 : 4 * lanes + 5]
    grads = refs[4 * lanes + 5 : 4 * lanes + 7]
    scaled_hidden = refs[4 * lanes + 7 : 4 * lanes + 9]
    rows = tok[0][0].shape[0]
    cols = gate_w.shape[1]
    mine = lax.axis_index("ep") % EPG
    rank = lax.axis_index("tp")
    spans = [
        pl.ds(pl.multiple_of(((rank + lanes - j) % lanes) * width, width), width)
        for j in range(lanes)
    ]
    lane = lax.broadcasted_iota(jnp.int32, (rows, LANES), 1)
    for c in range(2):
        pre_gate = jnp.zeros((rows, cols), F32)
        pre_up = jnp.zeros((rows, cols), F32)
        back = jnp.zeros((rows, cols), F32)
        for j in range(lanes):
            part = tok[c][j][...]
            pre_gate = pre_gate + dot(part, gate_w[spans[j], :], COLS_ROWS)
            pre_up = pre_up + dot(part, up_w[spans[j], :], COLS_ROWS)
            back = back + dot(cot[c][j][:, :width], down_w[:, spans[j]], ROWS_COLS)
        gates = cot[c][0][:, width:].astype(F32)
        gate = jnp.sum(jnp.where(lane == mine, gates, 0.0), axis=1, keepdims=True)
        sigma = jax.nn.sigmoid(pre_gate)
        swish = pre_gate * sigma
        hidden = swish * pre_up
        gate_part = jnp.sum(hidden * back, axis=1, keepdims=True)
        scaled = gate * back
        grad_gate = (scaled * pre_up * sigma * (1.0 + pre_gate * (1.0 - sigma))).astype(BF16)
        grad_up = (scaled * swish).astype(BF16)
        grads[c][:, :cols] = grad_gate
        grads[c][:, cols:] = grad_up
        scaled_hidden[c][...] = (gate * hidden).astype(BF16)
        for j in range(lanes):
            total = dot(grad_gate, gate_w[spans[j], :], ROWS_COLS)
            total = total + dot(grad_up, up_w[spans[j], :], ROWS_COLS)
            sums[c][:, j * width : (j + 1) * width] = total.astype(sums[c].dtype)
        high = gate_part.astype(BF16).astype(F32)
        low = gate_part - high
        tail = jnp.where(lane == mine, high, jnp.where(lane == mine + EPG, low, 0.0))
        sums[c][:, lanes * width :] = tail.astype(sums[c].dtype)


def up_body(lanes, width, *refs):
    tok = [refs[b * lanes : (b + 1) * lanes] for b in range(4)]
    grads = refs[4 * lanes : 4 * lanes + 4]
    gate_out, up_out = refs[4 * lanes + 4 :]
    cols = gate_out.shape[1]
    rank = lax.axis_index("tp")
    chunk = min(width, 512)
    for j in range(lanes):
        base = ((rank + lanes - j) % lanes) * width
        for s in range(0, width, chunk):
            span = pl.ds(pl.multiple_of(base + s, chunk), chunk)
            total = dot(tok[0][j][:, s : s + chunk], grads[0][...], ROWS_ROWS)
            for b in range(1, 4):
                total = total + dot(tok[b][j][:, s : s + chunk], grads[b][...], ROWS_ROWS)
            gate_out[span, :] = total[:, :cols]
            up_out[span, :] = total[:, cols:]


def down_body(lanes, width, *refs):
    cot = [refs[b * lanes : (b + 1) * lanes] for b in range(4)]
    scaled_hidden = refs[4 * lanes : 4 * lanes + 4]
    down_out = refs[4 * lanes + 4]
    rank = lax.axis_index("tp")
    chunk = min(width, 512)
    for j in range(lanes):
        base = ((rank + lanes - j) % lanes) * width
        for s in range(0, width, chunk):
            span = pl.ds(pl.multiple_of(base + s, chunk), chunk)
            down = dot(scaled_hidden[0][...], cot[0][j][:, s : s + chunk], ROWS_ROWS)
            for b in range(1, 4):
                down = down + dot(scaled_hidden[b][...], cot[b][j][:, s : s + chunk], ROWS_ROWS)
            down_out[:, span] = down


def final_body(groups, cap, *refs):
    back = refs[:groups]
    pick_refs = refs[groups : groups + 4]
    local_ref, weight_ref, expert_ref = refs[groups + 4 : groups + 7]
    tok_out, group_out, expert_out = refs[groups + 7 :]
    count, width = tok_out.shape
    picks = [pick_refs[min(k, 3)][pl.ds(max(k - 3, 0) * cap, cap), :] for k in range(groups)]
    total = jnp.zeros((count, width), F32)
    held = jnp.zeros((LANES, count), F32)
    for k in range(groups):
        total = total + dot(picks[k], back[k][:, :width], ROWS_ROWS)
        held = held + dot(back[k][:, width:], picks[k], ROWS_ROWS)
    tok_out[...] = total
    lane = lax.broadcasted_iota(jnp.int32, (LANES, count), 0)
    group_sum = jnp.zeros((1, count), F32)
    for k in range(local_ref.shape[0]):
        grad = jnp.sum(
            jnp.where(lane == local_ref[k : k + 1, :], held, 0.0), axis=0, keepdims=True
        )
        group_sum = group_sum + expert_ref[k : k + 1, :] * grad
        expert_out[k : k + 1, :] = weight_ref[...] * grad
    group_out[...] = group_sum


def layer(
    tokens, cotangent, group_weight, expert_weight, group_choice, local_choice, w_gate, w_up, w_down
):
    count, features = tokens.shape
    picks = expert_weight.shape[1]
    experts = lax.axis_size("ep")
    lanes = lax.axis_size("tp")
    groups = experts // EPG
    width = features // lanes
    capacity = picks * (3 * count // (2 * experts))
    cap = min(count, EPG * capacity // picks)
    cap = -(-cap // 16) * 16
    rows = groups * cap
    cols = w_gate.shape[2]

    def along_groups(a, k):
        return lax.ppermute(a, "ep", [(e, e ^ (k * EPG)) for e in range(experts)])

    def along_side(a):
        return lax.ppermute(a, "ep", [(e, e ^ 2) for e in range(experts)])

    def along_core(a):
        return lax.ppermute(a, "ep", [(e, e ^ 1) for e in range(experts)])

    def along_tp(a, j):
        return lax.ppermute(a, "tp", [(r, (r + j) % lanes) for r in range(lanes)])

    def along_both(a, j):
        pairs = [
            (e * lanes + r, (e ^ 2) * lanes + (r + j) % lanes)
            for e in range(experts)
            for r in range(lanes)
        ]
        return lax.ppermute(a, ("ep", "tp"), pairs)

    shape = jax.ShapeDtypeStruct
    choice_row = group_choice.reshape(1, count)
    weight_row = group_weight.reshape(1, count)
    local_rows = local_choice.T
    expert_rows = expert_weight.T
    routed = call(
        functools.partial(route_body, groups, cap, width),
        [shape((cap, 2 * width + LANES), BF16)]
        + [shape((cap, width), BF16)] * (groups - 1)
        + [shape((cap, width + LANES), BF16)] * (groups - 1),
        space=pltpu.HBM,
        scratch=[
            pltpu.VMEM((1, count), jnp.int32),
            pltpu.VMEM((picks, count), jnp.int32),
            pltpu.VMEM((1, count), F32),
            pltpu.VMEM((picks, count), F32),
            pltpu.VMEM((count, width), BF16),
            pltpu.VMEM((count, width), BF16),
            pltpu.SemaphoreType.DMA((6,)),
        ],
    )(
        *(
            pltpu.with_memory_space_constraint(a, pltpu.HBM)
            for a in (choice_row, local_rows, weight_row, expert_rows, tokens, cotangent)
        )
    )
    parts = [[0], [1], [2], list(range(3, groups))]
    picked = [
        call(
            functools.partial(picks_body, groups, cap, part),
            shape((len(part) * cap, count), BF16),
            10**6,
        )(choice_row)
        for part in parts
    ]
    own = routed[0]
    others = range(groups - 1, 0, -1)
    tok_sent = {k: along_groups(routed[k], k) for k in others}
    own_side = along_side(own)
    own_lane = [along_tp(own, j) for j in range(1, lanes)]
    cot_sent = {k: along_groups(routed[groups - 1 + k], k) for k in others}
    own_both = [along_both(own, j) for j in range(1, lanes)]
    tok = jnp.concatenate([tok_sent[k] for k in range(1, groups)], axis=0)
    cot = jnp.concatenate([cot_sent[k] for k in range(1, groups)], axis=0)
    cot_bare = jnp.concatenate([cot_sent[k][:, :width] for k in range(1, groups)], axis=0)
    tok_side = along_side(tok)
    tok_lane = [along_tp(tok, j) for j in range(1, lanes)]
    cot_side = along_side(cot)
    cot_lane = [along_tp(cot_bare, j) for j in range(1, lanes)]
    cut = width // 2 if width % (2 * LANES) == 0 else width

    def diagonal(side, lane):
        parts_a = [along_tp(side[:, :cut], j) for j in range(1, lanes)]
        if cut == width:
            return parts_a
        parts_b = [along_side(a[:, cut:width]) for a in lane]
        return [jnp.concatenate([a, b], axis=1) for a, b in zip(parts_a, parts_b)]

    tok_both = diagonal(tok_side, tok_lane)
    cot_both = diagonal(cot_side, cot_lane)

    def join(head, rest):
        return jnp.concatenate([head, rest], axis=0)

    tok_near = [join(own[:, :width], tok)]
    tok_near += [join(a[:, :width], b) for a, b in zip(own_lane, tok_lane)]
    cot_near = [join(own[:, width:], cot)]
    cot_near += [join(a[:, width : 2 * width], b) for a, b in zip(own_lane, cot_lane)]
    tok_far = [join(own_side[:, :width], tok_side)]
    tok_far += [join(a[:, :width], b) for a, b in zip(own_both, tok_both)]
    cot_far = [join(own_side[:, width:], cot_side)]
    cot_far += [join(a[:, width : 2 * width], b) for a, b in zip(own_both, cot_both)]
    first, second, third = w_gate[0], w_up[0], w_down[0]
    work = 2 * 5 * 2 * rows * features * cols

    def experts_on(tok_list, cot_list):
        tok_other = [along_core(a) for a in tok_list]
        cot_other = [along_core(a) for a in cot_list]
        outs = call(
            functools.partial(expert_body, lanes, width),
            [shape((rows, features + LANES), F32), shape((rows, features + LANES), BF16)]
            + [shape((rows, 2 * cols), BF16)] * 2
            + [shape((rows, cols), BF16)] * 2,
            work,
        )(*tok_list, *tok_other, *cot_list, *cot_other, first, second, third)
        return outs, tok_list + tok_other, cot_list + cot_other

    near, tok_a, cot_a = experts_on(tok_near, cot_near)
    far, tok_b, cot_b = experts_on(tok_far, cot_far)
    near_sum = near[0] + along_core(near[1]).astype(F32)
    far_sum = far[0] + along_core(far[1]).astype(F32)
    early = 3 * width // (8 * LANES) * LANES
    if lanes == 2 and early > 0:
        far_tail = far_sum[:, features:]
        near_in = along_tp(near_sum[:, width + early : features].astype(BF16), 1)
        lane_in = along_tp(far_sum[:, width + early : features].astype(BF16), 1)
        side_out = jnp.concatenate([far_sum[:, width : width + early], far_tail], axis=1)
        side_in = along_side(side_out.astype(BF16)).astype(F32)
        own_in = along_side(far_sum[:, :early].astype(BF16))
        last_in = along_side((far_sum[:, early:width] + lane_in.astype(F32)).astype(BF16))
        near_out = jnp.concatenate(
            [near_sum[:, width : width + early], near_sum[:, features:]], axis=1
        )
        next_out = near_out + side_in
        next_in = along_tp(next_out.astype(BF16), 1).astype(F32)
        tail = next_out[:, early:] + next_in[:, early:]
        head = near_sum[:, :early] + own_in.astype(F32) + next_in[:, :early]
        rest = near_sum[:, early:width] + near_in.astype(F32) + last_in.astype(F32)
        body = jnp.concatenate([head, rest], axis=1)
    else:
        both = near_sum + along_side(far_sum.astype(BF16)).astype(F32)
        tail = both[:, features:]
        body = both[:, :width]
        for j in range(1, lanes):
            piece = jnp.concatenate(
                [both[:, j * width : (j + 1) * width], both[:, features:]], axis=1
            )
            piece = along_tp(piece.astype(BF16), lanes - j).astype(F32)
            body = body + piece[:, :width]
            tail = tail + piece[:, width:]
    held = tail[:, :EPG] + tail[:, EPG : 2 * EPG]
    held = jnp.pad(held, ((0, 0), (0, LANES - EPG)))
    result = jnp.concatenate([body, held], axis=1).astype(BF16)
    sent = {k: along_groups(result[k * cap : (k + 1) * cap], k) for k in others}
    returned = [result[:cap]] + [sent[k] for k in range(1, groups)]
    grads = list(near[2:4]) + list(far[2:4])
    scaled_hidden = list(near[4:6]) + list(far[4:6])
    up_work = 2 * 2 * 4 * rows * features * cols
    first_grad, second_grad = call(
        functools.partial(up_body, lanes, width), [shape((features, cols), F32)] * 2, up_work
    )(*tok_a, *tok_b, *grads)
    third_grad = call(
        functools.partial(down_body, lanes, width), shape((cols, features), F32), up_work // 2
    )(*cot_a, *cot_b, *scaled_hidden)
    token_grad, group_grad, expert_grad = call(
        functools.partial(final_body, groups, cap),
        [shape((count, width), F32), shape((1, count), F32), shape((picks, count), F32)],
    )(*returned, *picked, local_rows, weight_row, expert_rows)
    return (
        token_grad,
        group_grad.reshape(count),
        expert_grad.T,
        first_grad[None],
        second_grad[None],
        third_grad[None],
    )


def solution(mesh):
    in_specs = (
        P("ep", None),
        P("ep", None),
        P("ep"),
        P("ep", None),
        P("ep"),
        P("ep", None),
        P("ep", None, "tp"),
        P("ep", None, "tp"),
        P("ep", "tp", None),
    )
    out_specs = (
        P("ep", "tp"),
        P("ep"),
        P("ep", None),
        P("ep", None, "tp"),
        P("ep", None, "tp"),
        P("ep", "tp", None),
    )
    return jax.shard_map(layer, mesh=mesh, in_specs=in_specs, out_specs=out_specs, check_vma=False)
```

```python
import functools

import jax
import jax.numpy as jnp
from jax import lax
from jax.experimental import pallas as pl
from jax.experimental.pallas import tpu as pltpu
from jax.sharding import PartitionSpec as P


EPG = 4
LANES = 128
F32 = jnp.float32
BF16 = jnp.bfloat16

ROWS_COLS = (((1,), (1,)), ((), ()))
COLS_ROWS = (((1,), (0,)), ((), ()))
ROWS_ROWS = (((0,), (0,)), ((), ()))


def dot(a, b, dims):
    return lax.dot_general(a, b, dims, preferred_element_type=F32)


def call(body, outs, flops=0, space=pltpu.VMEM, scratch=()):
    def run(*args):
        return pl.pallas_call(
            body,
            out_shape=outs,
            in_specs=[pl.BlockSpec(memory_space=space)] * len(args),
            out_specs=jax.tree.map(lambda _: pl.BlockSpec(memory_space=pltpu.VMEM), outs),
            scratch_shapes=scratch,
            compiler_params=pltpu.CompilerParams(vmem_limit_bytes=40 * 2**20),
            cost_estimate=pl.CostEstimate(flops=flops, bytes_accessed=0, transcendentals=0),
        )(*args)

    return run


def route_body(groups, cap, width, *refs):
    sources = refs[:6]
    whole_out = refs[6:8]
    tok_out = refs[8 : 6 + groups]
    cot_out = refs[6 + groups : 4 + 2 * groups]
    choice_ref, local_ref, weight_ref, expert_ref, tok_ref, cot_ref, sems = refs[4 + 2 * groups :]
    count = tok_ref.shape[0]
    own = lax.axis_index("ep") // EPG
    start = pl.multiple_of(lax.axis_index("tp") * width, width)
    copies = []
    for k, (src, dst) in enumerate(
        zip(sources, (choice_ref, local_ref, weight_ref, expert_ref, tok_ref, cot_ref))
    ):
        if k >= 4:
            src = src.at[:, pl.ds(start, width)]
        copies.append(pltpu.make_async_copy(src, dst, sems.at[k]))
    for copy in copies:
        copy.start()
    for copy in copies[:4]:
        copy.wait()
    choice = choice_ref[...]
    padded = -(-groups // 8) * 8
    member = lax.broadcasted_iota(jnp.int32, (padded, count), 0) == choice
    before = (
        lax.broadcasted_iota(jnp.int32, (count, count), 0)
        < lax.broadcasted_iota(jnp.int32, (count, count), 1)
    ).astype(BF16)
    member = member.astype(F32)
    ahead = dot(member.astype(BF16), before, COLS_ROWS)
    place = jnp.sum(ahead * member, axis=0, keepdims=True).astype(jnp.int32)
    lane = lax.broadcasted_iota(jnp.int32, (LANES, count), 0)
    gates = jnp.zeros((LANES, count), F32)
    for k in range(local_ref.shape[0]):
        gate = (weight_ref[...] * expert_ref[k : k + 1, :]).astype(BF16).astype(F32)
        gates = gates + jnp.where(lane == local_ref[k : k + 1, :], gate, 0.0)
    gates = gates.astype(BF16)
    slot = lax.broadcasted_iota(jnp.int32, (cap, count), 0)
    picks = [
        ((slot == place) & (choice == (own ^ k))).astype(F32).astype(BF16)
        for k in range(groups)
    ]
    gate_rows = [dot(pick, gates, ROWS_COLS).astype(BF16) for pick in picks]
    copies[4].wait()
    for k in range(groups):
        rows = dot(picks[k], tok_ref[...], COLS_ROWS).astype(BF16)
        if k < 2:
            whole_out[k][:, :width] = rows
        else:
            tok_out[k - 2][...] = rows
    copies[5].wait()
    for k in range(groups):
        rows = dot(picks[k], cot_ref[...], COLS_ROWS).astype(BF16)
        if k < 2:
            whole_out[k][:, width : 2 * width] = rows
            whole_out[k][:, 2 * width :] = gate_rows[k]
        else:
            cot_out[k - 2][:, :width] = rows
            cot_out[k - 2][:, width:] = gate_rows[k]


def picks_body(groups, cap, parts, choice_ref, out_ref):
    choice = choice_ref[...]
    count = choice.shape[1]
    own = lax.axis_index("ep") // EPG
    padded = -(-groups // 8) * 8
    member = (lax.broadcasted_iota(jnp.int32, (padded, count), 0) == choice).astype(F32)
    before = (
        lax.broadcasted_iota(jnp.int32, (count, count), 0)
        < lax.broadcasted_iota(jnp.int32, (count, count), 1)
    ).astype(BF16)
    ahead = dot(member.astype(BF16), before, COLS_ROWS)
    place = jnp.sum(ahead * member, axis=0, keepdims=True).astype(jnp.int32)
    slot = lax.broadcasted_iota(jnp.int32, (cap, count), 0)
    for i, k in enumerate(parts):
        pick = (slot == place) & (choice == (own ^ k))
        out_ref[pl.ds(i * cap, cap), :] = pick.astype(F32).astype(BF16)


def spans_of(lanes, width):
    rank = lax.axis_index("tp")
    return [
        pl.ds(pl.multiple_of(((rank + lanes - j) % lanes) * width, width), width)
        for j in range(lanes)
    ]


def pre_body(lanes, width, *refs):
    tok = [refs[c * lanes : (c + 1) * lanes] for c in range(2)]
    gate_w, up_w = refs[2 * lanes : 2 * lanes + 2]
    outs = refs[2 * lanes + 2 :]
    cols = gate_w.shape[1]
    spans = spans_of(lanes, width)
    for c in range(2):
        gate = dot(tok[c][0][...], gate_w[spans[0], :], COLS_ROWS)
        up = dot(tok[c][0][...], up_w[spans[0], :], COLS_ROWS)
        for j in range(1, lanes):
            gate = gate + dot(tok[c][j][...], gate_w[spans[j], :], COLS_ROWS)
            up = up + dot(tok[c][j][...], up_w[spans[j], :], COLS_ROWS)
        outs[c][:, :cols] = gate
        outs[c][:, cols:] = up


def main_body(lanes, width, *refs):
    pre = refs[:2]
    cot = [refs[2 + c * lanes : 2 + (c + 1) * lanes] for c in range(2)]
    gate_w, up_w, down_w = refs[2 + 2 * lanes : 5 + 2 * lanes]
    outs = refs[5 + 2 * lanes :]
    sums, grads, scaled_hidden = outs[:2], outs[2:4], outs[4:6]
    rows = pre[0].shape[0]
    cols = gate_w.shape[1]
    mine = lax.axis_index("ep") % EPG
    spans = spans_of(lanes, width)
    lane = lax.broadcasted_iota(jnp.int32, (rows, LANES), 1)
    for c in (1, 0):
        pre_gate = pre[c][:, :cols]
        pre_up = pre[c][:, cols:]
        back = dot(cot[c][0][:, :width], down_w[:, spans[0]], ROWS_COLS)
        for j in range(1, lanes):
            back = back + dot(cot[c][j][...], down_w[:, spans[j]], ROWS_COLS)
        gates = cot[c][0][:, width:].astype(F32)
        gate = jnp.sum(jnp.where(lane == mine, gates, 0.0), axis=1, keepdims=True)
        sigma = jax.nn.sigmoid(pre_gate)
        swish = pre_gate * sigma
        hidden = swish * pre_up
        gate_part = jnp.sum(hidden * back, axis=1, keepdims=True)
        scaled = gate * back
        grad_gate = (scaled * pre_up * sigma * (1.0 + pre_gate * (1.0 - sigma))).astype(BF16)
        grad_up = (scaled * swish).astype(BF16)
        grads[c][:, :cols] = grad_gate
        grads[c][:, cols:] = grad_up
        scaled_hidden[c][...] = (gate * hidden).astype(BF16)
        for j in range(1, lanes):
            total = dot(grad_gate, gate_w[spans[j], :], ROWS_COLS)
            total = total + dot(grad_up, up_w[spans[j], :], ROWS_COLS)
            sums[c][:, (j - 1) * width : j * width] = total.astype(sums[c].dtype)
        high = gate_part.astype(BF16).astype(F32)
        low = gate_part - high
        tail = jnp.where(lane == mine, high, jnp.where(lane == mine + EPG, low, 0.0))
        sums[c][:, (lanes - 1) * width :] = tail.astype(sums[c].dtype)


def own_body(lanes, width, *refs):
    grads, (gate_w, up_w), sums = refs[:2], refs[2:4], refs[4:]
    cols = gate_w.shape[1]
    span = spans_of(lanes, width)[0]
    for c in (1, 0):
        total = dot(grads[c][:, :cols], gate_w[span, :], ROWS_COLS)
        total = total + dot(grads[c][:, cols:], up_w[span, :], ROWS_COLS)
        sums[c][...] = total.astype(sums[c].dtype)


def up_body(lanes, width, *refs):
    tok = [refs[b * lanes : (b + 1) * lanes] for b in range(4)]
    grads = refs[4 * lanes : 4 * lanes + 4]
    gate_out, up_out = refs[4 * lanes + 4 :]
    cols = gate_out.shape[1]
    rank = lax.axis_index("tp")
    chunk = min(width, 512)
    for j in range(lanes):
        base = ((rank + lanes - j) % lanes) * width
        for s in range(0, width, chunk):
            span = pl.ds(pl.multiple_of(base + s, chunk), chunk)
            total = dot(tok[0][j][:, s : s + chunk], grads[0][...], ROWS_ROWS)
            for b in range(1, 4):
                total = total + dot(tok[b][j][:, s : s + chunk], grads[b][...], ROWS_ROWS)
            gate_out[span, :] = total[:, :cols]
            up_out[span, :] = total[:, cols:]


def down_body(lanes, width, *refs):
    cot = [refs[b * lanes : (b + 1) * lanes] for b in range(4)]
    scaled_hidden = refs[4 * lanes : 4 * lanes + 4]
    down_out = refs[4 * lanes + 4]
    rank = lax.axis_index("tp")
    chunk = min(width, 512)
    for j in range(lanes):
        base = ((rank + lanes - j) % lanes) * width
        for s in range(0, width, chunk):
            span = pl.ds(pl.multiple_of(base + s, chunk), chunk)
            down = dot(scaled_hidden[0][...], cot[0][j][:, s : s + chunk], ROWS_ROWS)
            for b in range(1, 4):
                down = down + dot(scaled_hidden[b][...], cot[b][j][:, s : s + chunk], ROWS_ROWS)
            down_out[:, span] = down


def final_body(groups, cap, *refs):
    back = refs[:groups]
    pick_refs = refs[groups : groups + 4]
    local_ref, weight_ref, expert_ref = refs[groups + 4 : groups + 7]
    tok_out, group_out, expert_out = refs[groups + 7 :]
    count, width = tok_out.shape
    picks = [pick_refs[min(k, 3)][pl.ds(max(k - 3, 0) * cap, cap), :] for k in range(groups)]
    total = jnp.zeros((count, width), F32)
    held = jnp.zeros((LANES, count), F32)
    for k in range(groups):
        total = total + dot(picks[k], back[k][:, :width], ROWS_ROWS)
        held = held + dot(back[k][:, width:], picks[k], ROWS_ROWS)
    tok_out[...] = total
    lane = lax.broadcasted_iota(jnp.int32, (LANES, count), 0)
    group_sum = jnp.zeros((1, count), F32)
    for k in range(local_ref.shape[0]):
        grad = jnp.sum(
            jnp.where(lane == local_ref[k : k + 1, :], held, 0.0), axis=0, keepdims=True
        )
        group_sum = group_sum + expert_ref[k : k + 1, :] * grad
        expert_out[k : k + 1, :] = weight_ref[...] * grad
    group_out[...] = group_sum


def layer(
    tokens, cotangent, group_weight, expert_weight, group_choice, local_choice, w_gate, w_up, w_down
):
    count, features = tokens.shape
    picks = expert_weight.shape[1]
    experts = lax.axis_size("ep")
    lanes = lax.axis_size("tp")
    groups = experts // EPG
    width = features // lanes
    capacity = picks * (3 * count // (2 * experts))
    cap = min(count, EPG * capacity // picks)
    cap = -(-cap // 16) * 16
    rows = groups * cap
    cols = w_gate.shape[2]

    def along_groups(a, k):
        return lax.ppermute(a, "ep", [(e, e ^ (k * EPG)) for e in range(experts)])

    def along_side(a):
        return lax.ppermute(a, "ep", [(e, e ^ 2) for e in range(experts)])

    def along_core(a):
        return lax.ppermute(a, "ep", [(e, e ^ 1) for e in range(experts)])

    def along_tp(a, j):
        return lax.ppermute(a, "tp", [(r, (r + j) % lanes) for r in range(lanes)])

    shape = jax.ShapeDtypeStruct
    choice_row = group_choice.reshape(1, count)
    weight_row = group_weight.reshape(1, count)
    local_rows = local_choice.T
    expert_rows = expert_weight.T
    routed = call(
        functools.partial(route_body, groups, cap, width),
        [shape((cap, 2 * width + LANES), BF16)] * 2
        + [shape((cap, width), BF16)] * (groups - 2)
        + [shape((cap, width + LANES), BF16)] * (groups - 2),
        space=pltpu.HBM,
        scratch=[
            pltpu.VMEM((1, count), jnp.int32),
            pltpu.VMEM((picks, count), jnp.int32),
            pltpu.VMEM((1, count), F32),
            pltpu.VMEM((picks, count), F32),
            pltpu.VMEM((count, width), BF16),
            pltpu.VMEM((count, width), BF16),
            pltpu.SemaphoreType.DMA((6,)),
        ],
    )(
        *(
            pltpu.with_memory_space_constraint(a, pltpu.HBM)
            for a in (choice_row, local_rows, weight_row, expert_rows, tokens, cotangent)
        )
    )
    parts = [[0], [1], [2], list(range(3, groups))]
    picked = [
        call(
            functools.partial(picks_body, groups, cap, part),
            shape((len(part) * cap, count), BF16),
            10**6,
        )(choice_row)
        for part in parts
    ]
    others = range(groups - 1, 1, -1)
    next_sent = along_groups(routed[1], 1)
    tok_sent = {k: along_groups(routed[k], k) for k in others}

    def join(head, rest):
        return jnp.concatenate([head, rest], axis=0)

    own_side = along_side(routed[0])
    own_lane = [along_tp(routed[0][:, : 2 * width], j) for j in range(1, lanes)]
    next_side = along_side(next_sent)
    next_lane = [along_tp(next_sent[:, : 2 * width], j) for j in range(1, lanes)]
    own = join(routed[0], next_sent)
    own_side = join(own_side, next_side)
    own_lane = [join(a, b) for a, b in zip(own_lane, next_lane)]
    cot_sent = {k: along_groups(routed[groups - 2 + k], k) for k in range(2, groups)}
    own_tok_both = [along_tp(own_side[:, :width], j) for j in range(1, lanes)]
    own_cot_both = [along_side(a[:, width:]) for a in own_lane]
    tok = jnp.concatenate([tok_sent[k] for k in range(2, groups)], axis=0)
    cot = jnp.concatenate([cot_sent[k] for k in range(2, groups)], axis=0)
    cot_bare = jnp.concatenate([cot_sent[k][:, :width] for k in range(2, groups)], axis=0)
    tok_side = along_side(tok)
    tok_lane = [along_tp(tok, j) for j in range(1, lanes)]
    cot_side = along_side(cot)
    cot_lane = [along_tp(cot_bare, j) for j in range(1, lanes)]
    cut = width // 2 if width % (2 * LANES) == 0 else width

    def diagonal(side, lane):
        parts_a = [along_tp(side[:, :cut], j) for j in range(1, lanes)]
        if cut == width:
            return parts_a
        parts_b = [along_side(a[:, cut:width]) for a in lane]
        return [jnp.concatenate([a, b], axis=1) for a, b in zip(parts_a, parts_b)]

    tok_both = diagonal(tok_side, tok_lane)
    cot_both = diagonal(cot_side, cot_lane)

    tok_near = [join(own[:, :width], tok)]
    tok_near += [join(a[:, :width], b) for a, b in zip(own_lane, tok_lane)]
    cot_near = [join(own[:, width:], cot)]
    cot_near += [join(a[:, width:], b) for a, b in zip(own_lane, cot_lane)]
    tok_far = [join(own_side[:, :width], tok_side)]
    tok_far += [join(a, b) for a, b in zip(own_tok_both, tok_both)]
    cot_far = [join(own_side[:, width:], cot_side)]
    cot_far += [join(a, b) for a, b in zip(own_cot_both, cot_both)]
    first, second, third = w_gate[0], w_up[0], w_down[0]
    work = 2 * 2 * rows * features * cols
    rest_width = features - width

    def experts_on(tok_list, cot_list):
        tok_other = [along_core(tok_list[0])]
        cot_other = [along_core(cot_list[0])]
        tok_other += [along_core(a) for a in tok_list[1:]]
        cot_other += [along_core(a) for a in cot_list[1:]]
        pre = call(
            functools.partial(pre_body, lanes, width), [shape((rows, 2 * cols), F32)] * 2, 2 * work
        )(*tok_list, *tok_other, first, second)
        outs = call(
            functools.partial(main_body, lanes, width),
            [shape((rows, rest_width + LANES), F32), shape((rows, rest_width + LANES), BF16)]
            + [shape((rows, 2 * cols), BF16)] * 2
            + [shape((rows, cols), BF16)] * 2,
            2 * work,
        )(*pre, *cot_list, *cot_other, first, second, third)
        rest = outs[0] + along_core(outs[1]).astype(F32)
        owned = call(
            functools.partial(own_body, lanes, width),
            [shape((rows, width), F32), shape((rows, width), BF16)],
            work,
        )(*outs[2:4], first, second)
        owned = owned[0] + along_core(owned[1]).astype(F32)
        return owned, rest, outs[2:4], outs[4:6], tok_list + tok_other, cot_list + cot_other

    near_own, near_rest, near_grads, near_hidden, tok_a, cot_a = experts_on(tok_near, cot_near)
    far_own, far_rest, far_grads, far_hidden, tok_b, cot_b = experts_on(tok_far, cot_far)
    early = 3 * width // (8 * LANES) * LANES
    if lanes == 2 and early > 0:
        near_in = along_tp(near_rest[:, early:width].astype(BF16), 1)
        lane_in = along_tp(far_rest[:, early:width].astype(BF16), 1)
        side_out = jnp.concatenate([far_rest[:, :early], far_rest[:, width:]], axis=1)
        side_in = along_side(side_out.astype(BF16)).astype(F32)
        own_in = along_side(far_own[:, :early].astype(BF16))
        last_in = along_side((far_own[:, early:] + lane_in.astype(F32)).astype(BF16))
        near_out = jnp.concatenate([near_rest[:, :early], near_rest[:, width:]], axis=1)
        next_out = near_out + side_in
        next_in = along_tp(next_out.astype(BF16), 1).astype(F32)
        tail = next_out[:, early:] + next_in[:, early:]
        head = near_own[:, :early] + own_in.astype(F32) + next_in[:, :early]
        rest = near_own[:, early:] + near_in.astype(F32) + last_in.astype(F32)
        body = jnp.concatenate([head, rest], axis=1)
    else:
        body = near_own + along_side(far_own.astype(BF16)).astype(F32)
        both = near_rest + along_side(far_rest.astype(BF16)).astype(F32)
        tail = both[:, rest_width:]
        for j in range(1, lanes):
            piece = jnp.concatenate(
                [both[:, (j - 1) * width : j * width], both[:, rest_width:]], axis=1
            )
            piece = along_tp(piece.astype(BF16), lanes - j).astype(F32)
            body = body + piece[:, :width]
            tail = tail + piece[:, width:]
    held = tail[:, :EPG] + tail[:, EPG : 2 * EPG]
    held = jnp.pad(held, ((0, 0), (0, LANES - EPG)))
    result = jnp.concatenate([body, held], axis=1).astype(BF16)
    sent = {k: along_groups(result[k * cap : (k + 1) * cap], k) for k in range(groups - 1, 0, -1)}
    returned = [result[:cap]] + [sent[k] for k in range(1, groups)]
    grads = list(near_grads) + list(far_grads)
    scaled_hidden = list(near_hidden) + list(far_hidden)
    up_work = 2 * 2 * 4 * rows * features * cols
    first_grad, second_grad = call(
        functools.partial(up_body, lanes, width), [shape((features, cols), F32)] * 2, up_work
    )(*tok_a, *tok_b, *grads)
    third_grad = call(
        functools.partial(down_body, lanes, width), shape((cols, features), F32), up_work // 2
    )(*cot_a, *cot_b, *scaled_hidden)
    token_grad, group_grad, expert_grad = call(
        functools.partial(final_body, groups, cap),
        [shape((count, width), F32), shape((1, count), F32), shape((picks, count), F32)],
    )(*returned, *picked, local_rows, weight_row, expert_rows)
    return (
        token_grad,
        group_grad.reshape(count),
        expert_grad.T,
        first_grad[None],
        second_grad[None],
        third_grad[None],
    )


def solution(mesh):
    in_specs = (
        P("ep", None),
        P("ep", None),
        P("ep"),
        P("ep", None),
        P("ep"),
        P("ep", None),
        P("ep", None, "tp"),
        P("ep", None, "tp"),
        P("ep", "tp", None),
    )
    out_specs = (
        P("ep", "tp"),
        P("ep"),
        P("ep", None),
        P("ep", None, "tp"),
        P("ep", None, "tp"),
        P("ep", "tp", None),
    )
    return jax.shard_map(layer, mesh=mesh, in_specs=in_specs, out_specs=out_specs, check_vma=False)
```

```python
import functools

import jax
import jax.numpy as jnp
from jax import lax
from jax.experimental import pallas as pl
from jax.experimental.pallas import tpu as pltpu
from jax.sharding import PartitionSpec as P


EPG = 4
LANES = 128
F32 = jnp.float32
BF16 = jnp.bfloat16

ROWS_COLS = (((1,), (1,)), ((), ()))
COLS_ROWS = (((1,), (0,)), ((), ()))
ROWS_ROWS = (((0,), (0,)), ((), ()))


def dot(a, b, dims):
    return lax.dot_general(a, b, dims, preferred_element_type=F32)


def call(body, outs, flops=0, space=pltpu.VMEM, scratch=()):
    def run(*args):
        return pl.pallas_call(
            body,
            out_shape=outs,
            in_specs=[pl.BlockSpec(memory_space=space)] * len(args),
            out_specs=jax.tree.map(lambda _: pl.BlockSpec(memory_space=pltpu.VMEM), outs),
            scratch_shapes=scratch,
            compiler_params=pltpu.CompilerParams(vmem_limit_bytes=40 * 2**20),
            cost_estimate=pl.CostEstimate(flops=flops, bytes_accessed=0, transcendentals=0),
        )(*args)

    return run


def route_body(groups, cap, width, *refs):
    sources = refs[:6]
    whole_out = refs[6:8]
    tok_out = refs[8 : 6 + groups]
    cot_out = refs[6 + groups : 4 + 2 * groups]
    choice_ref, local_ref, weight_ref, expert_ref, tok_ref, cot_ref, sems = refs[4 + 2 * groups :]
    count = tok_ref.shape[0]
    own = lax.axis_index("ep") // EPG
    start = pl.multiple_of(lax.axis_index("tp") * width, width)
    copies = []
    for k, (src, dst) in enumerate(
        zip(sources, (choice_ref, local_ref, weight_ref, expert_ref, tok_ref, cot_ref))
    ):
        if k >= 4:
            src = src.at[:, pl.ds(start, width)]
        copies.append(pltpu.make_async_copy(src, dst, sems.at[k]))
    for copy in copies:
        copy.start()
    for copy in copies[:4]:
        copy.wait()
    choice = choice_ref[...]
    padded = -(-groups // 8) * 8
    member = lax.broadcasted_iota(jnp.int32, (padded, count), 0) == choice
    before = (
        lax.broadcasted_iota(jnp.int32, (count, count), 0)
        < lax.broadcasted_iota(jnp.int32, (count, count), 1)
    ).astype(BF16)
    member = member.astype(F32)
    ahead = dot(member.astype(BF16), before, COLS_ROWS)
    place = jnp.sum(ahead * member, axis=0, keepdims=True).astype(jnp.int32)
    lane = lax.broadcasted_iota(jnp.int32, (LANES, count), 0)
    gates = jnp.zeros((LANES, count), F32)
    for k in range(local_ref.shape[0]):
        gate = (weight_ref[...] * expert_ref[k : k + 1, :]).astype(BF16).astype(F32)
        gates = gates + jnp.where(lane == local_ref[k : k + 1, :], gate, 0.0)
    gates = gates.astype(BF16)
    slot = lax.broadcasted_iota(jnp.int32, (cap, count), 0)
    picks = [
        ((slot == place) & (choice == (own ^ k))).astype(F32).astype(BF16)
        for k in range(groups)
    ]
    gate_rows = [dot(pick, gates, ROWS_COLS).astype(BF16) for pick in picks]
    copies[4].wait()
    for k in range(groups):
        rows = dot(picks[k], tok_ref[...], COLS_ROWS).astype(BF16)
        if k < 2:
            whole_out[k][:, :width] = rows
        else:
            tok_out[k - 2][...] = rows
    copies[5].wait()
    for k in range(groups):
        rows = dot(picks[k], cot_ref[...], COLS_ROWS).astype(BF16)
        if k < 2:
            whole_out[k][:, width : 2 * width] = rows
            whole_out[k][:, 2 * width :] = gate_rows[k]
        else:
            cot_out[k - 2][:, :width] = rows
            cot_out[k - 2][:, width:] = gate_rows[k]


def picks_body(groups, cap, parts, choice_ref, out_ref):
    choice = choice_ref[...]
    count = choice.shape[1]
    own = lax.axis_index("ep") // EPG
    padded = -(-groups // 8) * 8
    member = (lax.broadcasted_iota(jnp.int32, (padded, count), 0) == choice).astype(F32)
    before = (
        lax.broadcasted_iota(jnp.int32, (count, count), 0)
        < lax.broadcasted_iota(jnp.int32, (count, count), 1)
    ).astype(BF16)
    ahead = dot(member.astype(BF16), before, COLS_ROWS)
    place = jnp.sum(ahead * member, axis=0, keepdims=True).astype(jnp.int32)
    slot = lax.broadcasted_iota(jnp.int32, (cap, count), 0)
    for i, k in enumerate(parts):
        pick = (slot == place) & (choice == (own ^ k))
        out_ref[pl.ds(i * cap, cap), :] = pick.astype(F32).astype(BF16)


def spans_of(lanes, width):
    rank = lax.axis_index("tp")
    return [
        pl.ds(pl.multiple_of(((rank + lanes - j) % lanes) * width, width), width)
        for j in range(lanes)
    ]


def stack(parts):
    return jnp.concatenate(parts, axis=0)


def pre_body(lanes, width, *refs):
    tok = [refs[c * lanes : (c + 1) * lanes] for c in range(2)]
    gate_w, up_w, out = refs[2 * lanes :]
    cols = gate_w.shape[1]
    spans = spans_of(lanes, width)
    gate = up = 0.0
    for j in range(lanes):
        part = stack([tok[c][j][...] for c in range(2)])
        gate = gate + dot(part, gate_w[spans[j], :], COLS_ROWS)
        up = up + dot(part, up_w[spans[j], :], COLS_ROWS)
    out[:, :cols] = gate
    out[:, cols:] = up


def main_body(lanes, width, *refs):
    pre = refs[0]
    cot = [refs[1 + c * lanes : 1 + (c + 1) * lanes] for c in range(2)]
    gate_w, up_w, down_w = refs[1 + 2 * lanes : 4 + 2 * lanes]
    keep, send, grads, scaled_hidden = refs[4 + 2 * lanes :]
    rows = keep.shape[0]
    cols = gate_w.shape[1]
    mine = lax.axis_index("ep") % EPG
    spans = spans_of(lanes, width)
    lane = lax.broadcasted_iota(jnp.int32, (2 * rows, LANES), 1)
    pre_gate = pre[:, :cols]
    pre_up = pre[:, cols:]
    back = 0.0
    for j in range(lanes):
        part = stack([cot[c][j][:, :width] for c in range(2)])
        back = back + dot(part, down_w[:, spans[j]], ROWS_COLS)
    gates = stack([cot[c][0][:, width:] for c in range(2)]).astype(F32)
    gate = jnp.sum(jnp.where(lane == mine, gates, 0.0), axis=1, keepdims=True)
    sigma = jax.nn.sigmoid(pre_gate)
    swish = pre_gate * sigma
    hidden = swish * pre_up
    gate_part = jnp.sum(hidden * back, axis=1, keepdims=True)
    scaled = gate * back
    grad_gate = (scaled * pre_up * sigma * (1.0 + pre_gate * (1.0 - sigma))).astype(BF16)
    grad_up = (scaled * swish).astype(BF16)
    grads[:, :cols] = grad_gate
    grads[:, cols:] = grad_up
    scaled_hidden[...] = (gate * hidden).astype(BF16)
    for j in range(1, lanes):
        total = dot(grad_gate, gate_w[spans[j], :], ROWS_COLS)
        total = total + dot(grad_up, up_w[spans[j], :], ROWS_COLS)
        keep[:, (j - 1) * width : j * width] = total[:rows]
        send[:, (j - 1) * width : j * width] = total[rows:].astype(BF16)
    high = gate_part.astype(BF16).astype(F32)
    low = gate_part - high
    tail = jnp.where(lane == mine, high, jnp.where(lane == mine + EPG, low, 0.0))
    keep[:, (lanes - 1) * width :] = tail[:rows]
    send[:, (lanes - 1) * width :] = tail[rows:].astype(BF16)


def own_body(lanes, width, grads, gate_w, up_w, keep, send):
    rows = keep.shape[0]
    cols = gate_w.shape[1]
    span = spans_of(lanes, width)[0]
    total = dot(grads[:, :cols], gate_w[span, :], ROWS_COLS)
    total = total + dot(grads[:, cols:], up_w[span, :], ROWS_COLS)
    keep[...] = total[:rows]
    send[...] = total[rows:].astype(BF16)


def up_body(lanes, width, sets, *refs):
    tok = [refs[b * lanes : (b + 1) * lanes] for b in range(2 * sets)]
    grads = stack([ref[...] for ref in refs[2 * sets * lanes : 2 * sets * lanes + sets]])
    gate_out, up_out = refs[2 * sets * lanes + sets :]
    cols = gate_out.shape[1]
    rank = lax.axis_index("tp")
    chunk = min(width, 512)
    for j in range(lanes):
        base = ((rank + lanes - j) % lanes) * width
        for s in range(0, width, chunk):
            span = pl.ds(pl.multiple_of(base + s, chunk), chunk)
            part = stack([x[j][:, s : s + chunk] for x in tok])
            total = dot(part, grads, ROWS_ROWS)
            gate_out[span, :] = total[:, :cols]
            up_out[span, :] = total[:, cols:]


def down_body(lanes, width, sets, *refs):
    cot = [refs[b * lanes : (b + 1) * lanes] for b in range(2 * sets)]
    hidden = stack([ref[...] for ref in refs[2 * sets * lanes : 2 * sets * lanes + sets]])
    down_out = refs[2 * sets * lanes + sets]
    rank = lax.axis_index("tp")
    chunk = min(width, 512)
    for j in range(lanes):
        base = ((rank + lanes - j) % lanes) * width
        for s in range(0, width, chunk):
            span = pl.ds(pl.multiple_of(base + s, chunk), chunk)
            part = stack([x[j][:, s : s + chunk] for x in cot])
            down_out[:, span] = dot(hidden, part, ROWS_ROWS)


def final_body(groups, cap, *refs):
    back = refs[:groups]
    pick_refs = refs[groups : groups + 4]
    local_ref, weight_ref, expert_ref = refs[groups + 4 : groups + 7]
    tok_out, group_out, expert_out = refs[groups + 7 :]
    count, width = tok_out.shape
    picks = [pick_refs[min(k, 3)][pl.ds(max(k - 3, 0) * cap, cap), :] for k in range(groups)]
    total = jnp.zeros((count, width), F32)
    held = jnp.zeros((LANES, count), F32)
    for k in range(groups):
        total = total + dot(picks[k], back[k][:, :width], ROWS_ROWS)
        held = held + dot(back[k][:, width:], picks[k], ROWS_ROWS)
    tok_out[...] = total
    lane = lax.broadcasted_iota(jnp.int32, (LANES, count), 0)
    group_sum = jnp.zeros((1, count), F32)
    for k in range(local_ref.shape[0]):
        grad = jnp.sum(
            jnp.where(lane == local_ref[k : k + 1, :], held, 0.0), axis=0, keepdims=True
        )
        group_sum = group_sum + expert_ref[k : k + 1, :] * grad
        expert_out[k : k + 1, :] = weight_ref[...] * grad
    group_out[...] = group_sum


def layer(
    tokens, cotangent, group_weight, expert_weight, group_choice, local_choice, w_gate, w_up, w_down
):
    count, features = tokens.shape
    picks = expert_weight.shape[1]
    experts = lax.axis_size("ep")
    lanes = lax.axis_size("tp")
    groups = experts // EPG
    width = features // lanes
    capacity = picks * (3 * count // (2 * experts))
    cap = min(count, EPG * capacity // picks)
    cap = -(-cap // 16) * 16
    rows = groups * cap
    cols = w_gate.shape[2]

    def along_groups(a, k):
        return lax.ppermute(a, "ep", [(e, e ^ (k * EPG)) for e in range(experts)])

    def along_side(a):
        return lax.ppermute(a, "ep", [(e, e ^ 2) for e in range(experts)])

    def along_core(a):
        return lax.ppermute(a, "ep", [(e, e ^ 1) for e in range(experts)])

    def along_tp(a, j):
        return lax.ppermute(a, "tp", [(r, (r + j) % lanes) for r in range(lanes)])

    core = lax.axis_index("ep") % 2

    def along_diagonal(side, lane):
        pieces = []
        for j, a in enumerate(lane, 1):
            pairs = []
            for e in range(experts):
                for r in range(lanes):
                    there = (e ^ 2) * lanes + r if e % 2 else e * lanes + (r + j) % lanes
                    pairs.append((e * lanes + r, there))
            pieces.append(lax.ppermute(jnp.where(core == 0, side, a), ("ep", "tp"), pairs))
        return pieces

    shape = jax.ShapeDtypeStruct
    choice_row = group_choice.reshape(1, count)
    weight_row = group_weight.reshape(1, count)
    local_rows = local_choice.T
    expert_rows = expert_weight.T
    routed = call(
        functools.partial(route_body, groups, cap, width),
        [shape((cap, 2 * width + LANES), BF16)] * 2
        + [shape((cap, width), BF16)] * (groups - 2)
        + [shape((cap, width + LANES), BF16)] * (groups - 2),
        space=pltpu.HBM,
        scratch=[
            pltpu.VMEM((1, count), jnp.int32),
            pltpu.VMEM((picks, count), jnp.int32),
            pltpu.VMEM((1, count), F32),
            pltpu.VMEM((picks, count), F32),
            pltpu.VMEM((count, width), BF16),
            pltpu.VMEM((count, width), BF16),
            pltpu.SemaphoreType.DMA((6,)),
        ],
    )(
        *(
            pltpu.with_memory_space_constraint(a, pltpu.HBM)
            for a in (choice_row, local_rows, weight_row, expert_rows, tokens, cotangent)
        )
    )
    parts = [[0], [1], [2], list(range(3, groups))]
    picked = [
        call(
            functools.partial(picks_body, groups, cap, part),
            shape((len(part) * cap, count), BF16),
            10**6,
        )(choice_row)
        for part in parts
    ]
    others = range(groups - 1, 1, -1)
    next_sent = along_groups(routed[1], 1)
    tok_sent = {k: along_groups(routed[k], k) for k in others}

    def join(head, rest):
        return jnp.concatenate([head, rest], axis=0)

    own_side = along_side(routed[0])
    own_lane = [along_tp(routed[0][:, : 2 * width], j) for j in range(1, lanes)]
    next_side = along_side(next_sent)
    next_lane = [along_tp(next_sent[:, : 2 * width], j) for j in range(1, lanes)]
    own = join(routed[0], next_sent)
    own_side = join(own_side, next_side)
    own_lane = [join(a, b) for a, b in zip(own_lane, next_lane)]
    cot_sent = {k: along_groups(routed[groups - 2 + k], k) for k in range(2, groups)}
    own_both = along_diagonal(own_side[:, : 2 * width], own_lane)
    tok = jnp.concatenate([tok_sent[k] for k in range(2, groups)], axis=0)
    cot = jnp.concatenate([cot_sent[k] for k in range(2, groups)], axis=0)
    cot_bare = jnp.concatenate([cot_sent[k][:, :width] for k in range(2, groups)], axis=0)
    tok_side = along_side(tok)
    tok_lane = [along_tp(tok, j) for j in range(1, lanes)]
    cot_side = along_side(cot)
    cot_lane = [along_tp(cot_bare, j) for j in range(1, lanes)]
    tok_both = along_diagonal(tok_side, tok_lane)
    cot_both = along_diagonal(cot_side[:, :width], cot_lane)

    tok_near = [join(own[:, :width], tok)]
    tok_near += [join(a[:, :width], b) for a, b in zip(own_lane, tok_lane)]
    cot_near = [join(own[:, width:], cot)]
    cot_near += [join(a[:, width:], b) for a, b in zip(own_lane, cot_lane)]
    tok_far = [join(own_side[:, :width], tok_side)]
    tok_far += [join(a[:, :width], b) for a, b in zip(own_both, tok_both)]
    cot_far = [join(own_side[:, width:], cot_side)]
    cot_far += [join(a[:, width:], b) for a, b in zip(own_both, cot_both)]
    first, second, third = w_gate[0], w_up[0], w_down[0]
    rest_width = features - width

    def experts_on(tok_list, cot_list):
        size = tok_list[0].shape[0]
        work = 2 * 2 * size * features * cols
        tok_other = [along_core(tok_list[0])]
        cot_other = [along_core(cot_list[0])]
        tok_other += [along_core(a) for a in tok_list[1:]]
        cot_other += [along_core(a) for a in cot_list[1:]]
        pre = call(
            functools.partial(pre_body, lanes, width), shape((2 * size, 2 * cols), F32), 2 * work
        )(*tok_list, *tok_other, first, second)
        outs = call(
            functools.partial(main_body, lanes, width),
            [shape((size, rest_width + LANES), F32), shape((size, rest_width + LANES), BF16)]
            + [shape((2 * size, 2 * cols), BF16), shape((2 * size, cols), BF16)],
            2 * work,
        )(pre, *cot_list, *cot_other, first, second, third)
        rest = outs[0] + along_core(outs[1]).astype(F32)
        owned = call(
            functools.partial(own_body, lanes, width),
            [shape((size, width), F32), shape((size, width), BF16)],
            work,
        )(outs[2], first, second)
        owned = owned[0] + along_core(owned[1]).astype(F32)
        return owned, rest, [outs[2]], [outs[3]], tok_list + tok_other, cot_list + cot_other

    near_own, near_rest, *near = experts_on(tok_near, cot_near)
    far_own, far_rest, *far = experts_on(tok_far, cot_far)
    early = 3 * width // (8 * LANES) * LANES
    if lanes == 2 and early > 0:
        near_in = along_tp(near_rest[:, early:width].astype(BF16), 1)
        lane_in = along_tp(far_rest[:, early:width].astype(BF16), 1)
        side_out = jnp.concatenate([far_rest[:, :early], far_rest[:, width:]], axis=1)
        side_in = along_side(side_out.astype(BF16)).astype(F32)
        own_in = along_side(far_own[:, :early].astype(BF16))
        last_in = along_side((far_own[:, early:] + lane_in.astype(F32)).astype(BF16))
        near_out = jnp.concatenate([near_rest[:, :early], near_rest[:, width:]], axis=1)
        next_out = near_out + side_in
        next_in = along_tp(next_out.astype(BF16), 1).astype(F32)
        tail = next_out[:, early:] + next_in[:, early:]
        left = near_own[:, :early] + own_in.astype(F32) + next_in[:, :early]
        right = near_own[:, early:] + near_in.astype(F32) + last_in.astype(F32)
        body = jnp.concatenate([left, right], axis=1)
    else:
        body = near_own + along_side(far_own.astype(BF16)).astype(F32)
        both = near_rest + along_side(far_rest.astype(BF16)).astype(F32)
        tail = both[:, rest_width:]
        for j in range(1, lanes):
            piece = jnp.concatenate(
                [both[:, (j - 1) * width : j * width], both[:, rest_width:]], axis=1
            )
            piece = along_tp(piece.astype(BF16), lanes - j).astype(F32)
            body = body + piece[:, :width]
            tail = tail + piece[:, width:]
    held = tail[:, :EPG] + tail[:, EPG : 2 * EPG]
    held = jnp.pad(held, ((0, 0), (0, LANES - EPG)))
    result = jnp.concatenate([body, held], axis=1).astype(BF16)
    sent = {k: along_groups(result[k * cap : (k + 1) * cap], k) for k in range(groups - 1, 0, -1)}
    returned = [result[:cap]] + [sent[k] for k in range(1, groups)]
    grads, scaled_hidden, toks, cots = [near[i] + far[i] for i in range(4)]
    up_work = 2 * 2 * 4 * rows * features * cols
    first_grad, second_grad = call(
        functools.partial(up_body, lanes, width, len(grads)),
        [shape((features, cols), F32)] * 2,
        up_work,
    )(*toks, *grads)
    third_grad = call(
        functools.partial(down_body, lanes, width, len(grads)),
        shape((cols, features), F32),
        up_work // 2,
    )(*cots, *scaled_hidden)
    token_grad, group_grad, expert_grad = call(
        functools.partial(final_body, groups, cap),
        [shape((count, width), F32), shape((1, count), F32), shape((picks, count), F32)],
    )(*returned, *picked, local_rows, weight_row, expert_rows)
    return (
        token_grad,
        group_grad.reshape(count),
        expert_grad.T,
        first_grad[None],
        second_grad[None],
        third_grad[None],
    )


def solution(mesh):
    in_specs = (
        P("ep", None),
        P("ep", None),
        P("ep"),
        P("ep", None),
        P("ep"),
        P("ep", None),
        P("ep", None, "tp"),
        P("ep", None, "tp"),
        P("ep", "tp", None),
    )
    out_specs = (
        P("ep", "tp"),
        P("ep"),
        P("ep", None),
        P("ep", None, "tp"),
        P("ep", None, "tp"),
        P("ep", "tp", None),
    )
    return jax.shard_map(layer, mesh=mesh, in_specs=in_specs, out_specs=out_specs, check_vma=False)
```

```python
import functools

import jax
import jax.numpy as jnp
from jax import lax
from jax.experimental import pallas as pl
from jax.experimental.pallas import tpu as pltpu
from jax.sharding import PartitionSpec as P


EPG = 4
LANES = 128
F32 = jnp.float32
BF16 = jnp.bfloat16

ROWS_COLS = (((1,), (1,)), ((), ()))
COLS_ROWS = (((1,), (0,)), ((), ()))
ROWS_ROWS = (((0,), (0,)), ((), ()))


def dot(a, b, dims):
    return lax.dot_general(a, b, dims, preferred_element_type=F32)


def call(body, outs, flops=0, space=pltpu.VMEM, scratch=()):
    def run(*args):
        return pl.pallas_call(
            body,
            out_shape=outs,
            in_specs=[pl.BlockSpec(memory_space=space)] * len(args),
            out_specs=jax.tree.map(lambda _: pl.BlockSpec(memory_space=pltpu.VMEM), outs),
            scratch_shapes=scratch,
            compiler_params=pltpu.CompilerParams(vmem_limit_bytes=40 * 2**20),
            cost_estimate=pl.CostEstimate(flops=flops, bytes_accessed=0, transcendentals=0),
        )(*args)

    return run


def route_body(groups, cap, width, *refs):
    sources = refs[:6]
    whole_out = refs[6:8]
    tok_out = refs[8 : 6 + groups]
    cot_out = refs[6 + groups : 4 + 2 * groups]
    choice_ref, local_ref, weight_ref, expert_ref, tok_ref, cot_ref, sems = refs[4 + 2 * groups :]
    count = tok_ref.shape[0]
    own = lax.axis_index("ep") // EPG
    start = pl.multiple_of(lax.axis_index("tp") * width, width)
    copies = []
    for k, (src, dst) in enumerate(
        zip(sources, (choice_ref, local_ref, weight_ref, expert_ref, tok_ref, cot_ref))
    ):
        if k >= 4:
            src = src.at[:, pl.ds(start, width)]
        copies.append(pltpu.make_async_copy(src, dst, sems.at[k]))
    for copy in copies:
        copy.start()
    for copy in copies[:4]:
        copy.wait()
    choice = choice_ref[...]
    padded = -(-groups // 8) * 8
    member = lax.broadcasted_iota(jnp.int32, (padded, count), 0) == choice
    before = (
        lax.broadcasted_iota(jnp.int32, (count, count), 0)
        < lax.broadcasted_iota(jnp.int32, (count, count), 1)
    ).astype(BF16)
    member = member.astype(F32)
    ahead = dot(member.astype(BF16), before, COLS_ROWS)
    place = jnp.sum(ahead * member, axis=0, keepdims=True).astype(jnp.int32)
    lane = lax.broadcasted_iota(jnp.int32, (LANES, count), 0)
    gates = jnp.zeros((LANES, count), F32)
    for k in range(local_ref.shape[0]):
        gate = (weight_ref[...] * expert_ref[k : k + 1, :]).astype(BF16).astype(F32)
        gates = gates + jnp.where(lane == local_ref[k : k + 1, :], gate, 0.0)
    gates = gates.astype(BF16)
    slot = lax.broadcasted_iota(jnp.int32, (cap, count), 0)
    picks = [
        ((slot == place) & (choice == (own ^ k))).astype(F32).astype(BF16)
        for k in range(groups)
    ]
    gate_rows = [dot(pick, gates, ROWS_COLS).astype(BF16) for pick in picks]
    copies[4].wait()
    for k in range(groups):
        rows = dot(picks[k], tok_ref[...], COLS_ROWS).astype(BF16)
        if k < 2:
            whole_out[k][:, :width] = rows
        else:
            tok_out[k - 2][...] = rows
    copies[5].wait()
    for k in range(groups):
        rows = dot(picks[k], cot_ref[...], COLS_ROWS).astype(BF16)
        if k < 2:
            whole_out[k][:, width : 2 * width] = rows
            whole_out[k][:, 2 * width :] = gate_rows[k]
        else:
            cot_out[k - 2][:, :width] = rows
            cot_out[k - 2][:, width:] = gate_rows[k]


def picks_body(groups, cap, parts, choice_ref, out_ref):
    choice = choice_ref[...]
    count = choice.shape[1]
    own = lax.axis_index("ep") // EPG
    padded = -(-groups // 8) * 8
    member = (lax.broadcasted_iota(jnp.int32, (padded, count), 0) == choice).astype(F32)
    before = (
        lax.broadcasted_iota(jnp.int32, (count, count), 0)
        < lax.broadcasted_iota(jnp.int32, (count, count), 1)
    ).astype(BF16)
    ahead = dot(member.astype(BF16), before, COLS_ROWS)
    place = jnp.sum(ahead * member, axis=0, keepdims=True).astype(jnp.int32)
    slot = lax.broadcasted_iota(jnp.int32, (cap, count), 0)
    for i, k in enumerate(parts):
        pick = (slot == place) & (choice == (own ^ k))
        out_ref[pl.ds(i * cap, cap), :] = pick.astype(F32).astype(BF16)


def spans_of(lanes, width):
    rank = lax.axis_index("tp")
    return [
        pl.ds(pl.multiple_of(((rank + lanes - j) % lanes) * width, width), width)
        for j in range(lanes)
    ]


def stack(parts):
    return jnp.concatenate(parts, axis=0)


def pre_body(lanes, width, *refs):
    tok = [refs[c * lanes : (c + 1) * lanes] for c in range(2)]
    gate_w, up_w, out = refs[2 * lanes :]
    cols = gate_w.shape[1]
    spans = spans_of(lanes, width)
    gate = up = 0.0
    for j in range(lanes):
        part = stack([tok[c][j][...] for c in range(2)])
        gate = gate + dot(part, gate_w[spans[j], :], COLS_ROWS)
        up = up + dot(part, up_w[spans[j], :], COLS_ROWS)
    sigma = jax.nn.sigmoid(gate)
    swish = gate * sigma
    out[:, :cols] = swish
    out[:, cols : 2 * cols] = swish * up
    out[:, 2 * cols :] = up * sigma * (1.0 + gate * (1.0 - sigma))


def main_body(lanes, width, *refs):
    pre = refs[0]
    cot = [refs[1 + c * lanes : 1 + (c + 1) * lanes] for c in range(2)]
    gate_w, up_w, down_w = refs[1 + 2 * lanes : 4 + 2 * lanes]
    keep, send, grads, scaled_hidden = refs[4 + 2 * lanes :]
    rows = keep.shape[0]
    cols = gate_w.shape[1]
    mine = lax.axis_index("ep") % EPG
    spans = spans_of(lanes, width)
    lane = lax.broadcasted_iota(jnp.int32, (2 * rows, LANES), 1)
    back = 0.0
    for j in range(lanes):
        part = stack([cot[c][j][:, :width] for c in range(2)])
        back = back + dot(part, down_w[:, spans[j]], ROWS_COLS)
    gates = stack([cot[c][0][:, width:] for c in range(2)]).astype(F32)
    gate = jnp.sum(jnp.where(lane == mine, gates, 0.0), axis=1, keepdims=True)
    hidden = pre[:, cols : 2 * cols]
    gate_part = jnp.sum(hidden * back, axis=1, keepdims=True)
    scaled = gate * back
    grad_gate = (scaled * pre[:, 2 * cols :]).astype(BF16)
    grad_up = (scaled * pre[:, :cols]).astype(BF16)
    grads[:, :cols] = grad_gate
    grads[:, cols:] = grad_up
    scaled_hidden[...] = (gate * hidden).astype(BF16)
    for j in range(1, lanes):
        total = dot(grad_gate, gate_w[spans[j], :], ROWS_COLS)
        total = total + dot(grad_up, up_w[spans[j], :], ROWS_COLS)
        keep[:, (j - 1) * width : j * width] = total[:rows]
        send[:, (j - 1) * width : j * width] = total[rows:].astype(BF16)
    high = gate_part.astype(BF16).astype(F32)
    low = gate_part - high
    tail = jnp.where(lane == mine, high, jnp.where(lane == mine + EPG, low, 0.0))
    keep[:, (lanes - 1) * width :] = tail[:rows]
    send[:, (lanes - 1) * width :] = tail[rows:].astype(BF16)


def own_body(lanes, width, grads, gate_w, up_w, keep, send):
    rows = keep.shape[0]
    cols = gate_w.shape[1]
    span = spans_of(lanes, width)[0]
    total = dot(grads[:, :cols], gate_w[span, :], ROWS_COLS)
    total = total + dot(grads[:, cols:], up_w[span, :], ROWS_COLS)
    keep[...] = total[:rows]
    send[...] = total[rows:].astype(BF16)


def up_body(lanes, width, sets, *refs):
    tok = [refs[b * lanes : (b + 1) * lanes] for b in range(2 * sets)]
    grads = stack([ref[...] for ref in refs[2 * sets * lanes : 2 * sets * lanes + sets]])
    gate_out, up_out = refs[2 * sets * lanes + sets :]
    cols = gate_out.shape[1]
    rank = lax.axis_index("tp")
    chunk = min(width, 512)
    for j in range(lanes):
        base = ((rank + lanes - j) % lanes) * width
        for s in range(0, width, chunk):
            span = pl.ds(pl.multiple_of(base + s, chunk), chunk)
            part = stack([x[j][:, s : s + chunk] for x in tok])
            total = dot(part, grads, ROWS_ROWS)
            gate_out[span, :] = total[:, :cols]
            up_out[span, :] = total[:, cols:]


def down_body(lanes, width, sets, *refs):
    cot = [refs[b * lanes : (b + 1) * lanes] for b in range(2 * sets)]
    hidden = stack([ref[...] for ref in refs[2 * sets * lanes : 2 * sets * lanes + sets]])
    down_out = refs[2 * sets * lanes + sets]
    rank = lax.axis_index("tp")
    chunk = min(width, 512)
    for j in range(lanes):
        base = ((rank + lanes - j) % lanes) * width
        for s in range(0, width, chunk):
            span = pl.ds(pl.multiple_of(base + s, chunk), chunk)
            part = stack([x[j][:, s : s + chunk] for x in cot])
            down_out[:, span] = dot(hidden, part, ROWS_ROWS)


def final_body(groups, cap, *refs):
    back = refs[:groups]
    pick_refs = refs[groups : groups + 4]
    local_ref, weight_ref, expert_ref = refs[groups + 4 : groups + 7]
    tok_out, group_out, expert_out = refs[groups + 7 :]
    count, width = tok_out.shape
    picks = [pick_refs[min(k, 3)][pl.ds(max(k - 3, 0) * cap, cap), :] for k in range(groups)]
    total = jnp.zeros((count, width), F32)
    held = jnp.zeros((LANES, count), F32)
    for k in range(groups):
        total = total + dot(picks[k], back[k][:, :width], ROWS_ROWS)
        held = held + dot(back[k][:, width:], picks[k], ROWS_ROWS)
    tok_out[...] = total
    lane = lax.broadcasted_iota(jnp.int32, (LANES, count), 0)
    group_sum = jnp.zeros((1, count), F32)
    for k in range(local_ref.shape[0]):
        grad = jnp.sum(
            jnp.where(lane == local_ref[k : k + 1, :], held, 0.0), axis=0, keepdims=True
        )
        group_sum = group_sum + expert_ref[k : k + 1, :] * grad
        expert_out[k : k + 1, :] = weight_ref[...] * grad
    group_out[...] = group_sum


def layer(
    tokens, cotangent, group_weight, expert_weight, group_choice, local_choice, w_gate, w_up, w_down
):
    count, features = tokens.shape
    picks = expert_weight.shape[1]
    experts = lax.axis_size("ep")
    lanes = lax.axis_size("tp")
    groups = experts // EPG
    width = features // lanes
    capacity = picks * (3 * count // (2 * experts))
    cap = min(count, EPG * capacity // picks)
    cap = -(-cap // 16) * 16
    rows = groups * cap
    cols = w_gate.shape[2]

    def along_groups(a, k):
        return lax.ppermute(a, "ep", [(e, e ^ (k * EPG)) for e in range(experts)])

    def along_side(a):
        return lax.ppermute(a, "ep", [(e, e ^ 2) for e in range(experts)])

    def along_core(a):
        return lax.ppermute(a, "ep", [(e, e ^ 1) for e in range(experts)])

    def along_tp(a, j):
        return lax.ppermute(a, "tp", [(r, (r + j) % lanes) for r in range(lanes)])

    core = lax.axis_index("ep") % 2

    def along_diagonal(side, lane):
        pieces = []
        for j, a in enumerate(lane, 1):
            pairs = []
            for e in range(experts):
                for r in range(lanes):
                    there = (e ^ 2) * lanes + r if e % 2 else e * lanes + (r + j) % lanes
                    pairs.append((e * lanes + r, there))
            pieces.append(lax.ppermute(jnp.where(core == 0, side, a), ("ep", "tp"), pairs))
        return pieces

    shape = jax.ShapeDtypeStruct
    choice_row = group_choice.reshape(1, count)
    weight_row = group_weight.reshape(1, count)
    local_rows = local_choice.T
    expert_rows = expert_weight.T
    routed = call(
        functools.partial(route_body, groups, cap, width),
        [shape((cap, 2 * width + LANES), BF16)] * 2
        + [shape((cap, width), BF16)] * (groups - 2)
        + [shape((cap, width + LANES), BF16)] * (groups - 2),
        space=pltpu.HBM,
        scratch=[
            pltpu.VMEM((1, count), jnp.int32),
            pltpu.VMEM((picks, count), jnp.int32),
            pltpu.VMEM((1, count), F32),
            pltpu.VMEM((picks, count), F32),
            pltpu.VMEM((count, width), BF16),
            pltpu.VMEM((count, width), BF16),
            pltpu.SemaphoreType.DMA((6,)),
        ],
    )(
        *(
            pltpu.with_memory_space_constraint(a, pltpu.HBM)
            for a in (choice_row, local_rows, weight_row, expert_rows, tokens, cotangent)
        )
    )
    parts = [[0], [1], [2], list(range(3, groups))]
    picked = [
        call(
            functools.partial(picks_body, groups, cap, part),
            shape((len(part) * cap, count), BF16),
            10**6,
        )(choice_row)
        for part in parts
    ]
    others = range(groups - 1, 1, -1)
    next_sent = along_groups(routed[1], 1)
    tok_sent = {k: along_groups(routed[k], k) for k in others}

    def join(head, rest):
        return jnp.concatenate([head, rest], axis=0)

    def along_mixed(a, flip):
        pairs = []
        for e in range(experts):
            for r in range(lanes):
                across = (e + flip) % 2
                there = (e ^ 2) * lanes + r if across else e * lanes + (r + 1) % lanes
                pairs.append((e * lanes + r, there))
        return lax.ppermute(a, ("ep", "tp"), pairs)

    next_side = along_side(next_sent)
    next_lane = [along_tp(next_sent[:, : 2 * width], j) for j in range(1, lanes)]
    if lanes == 2:
        step = along_mixed(routed[0], 1)
        steps = along_mixed(join(routed[0], step), 0)
        own_side = jnp.where(core == 0, step, steps[:cap])
        own_lane = [jnp.where(core == 0, steps[:cap], step)[:, : 2 * width]]
        own_both = [steps[cap:, : 2 * width]]
        next_both = along_diagonal(next_side[:, : 2 * width], next_lane)
    else:
        own_side = along_side(routed[0])
        own_lane = [along_tp(routed[0][:, : 2 * width], j) for j in range(1, lanes)]
        own_both = along_diagonal(own_side[:, : 2 * width], own_lane)
        next_both = along_diagonal(next_side[:, : 2 * width], next_lane)
    own = join(routed[0], next_sent)
    own_side = join(own_side, next_side)
    own_lane = [join(a, b) for a, b in zip(own_lane, next_lane)]
    own_both = [join(a, b) for a, b in zip(own_both, next_both)]
    cot_sent = {k: along_groups(routed[groups - 2 + k], k) for k in range(2, groups)}
    tok = jnp.concatenate([tok_sent[k] for k in range(2, groups)], axis=0)
    cot = jnp.concatenate([cot_sent[k] for k in range(2, groups)], axis=0)
    cot_bare = jnp.concatenate([cot_sent[k][:, :width] for k in range(2, groups)], axis=0)
    tok_side = along_side(tok)
    tok_lane = [along_tp(tok, j) for j in range(1, lanes)]
    cot_side = along_side(cot)
    cot_lane = [along_tp(cot_bare, j) for j in range(1, lanes)]
    tok_both = along_diagonal(tok_side, tok_lane)
    cot_both = along_diagonal(cot_side[:, :width], cot_lane)

    tok_near = [join(own[:, :width], tok)]
    tok_near += [join(a[:, :width], b) for a, b in zip(own_lane, tok_lane)]
    cot_near = [join(own[:, width:], cot)]
    cot_near += [join(a[:, width:], b) for a, b in zip(own_lane, cot_lane)]
    tok_far = [join(own_side[:, :width], tok_side)]
    tok_far += [join(a[:, :width], b) for a, b in zip(own_both, tok_both)]
    cot_far = [join(own_side[:, width:], cot_side)]
    cot_far += [join(a[:, width:], b) for a, b in zip(own_both, cot_both)]
    first, second, third = w_gate[0], w_up[0], w_down[0]
    rest_width = features - width

    def experts_on(tok_list, cot_list):
        size = tok_list[0].shape[0]
        work = 2 * 2 * size * features * cols
        tok_other = [along_core(tok_list[0])]
        cot_other = [along_core(cot_list[0])]
        tok_other += [along_core(a) for a in tok_list[1:]]
        cot_other += [along_core(a) for a in cot_list[1:]]
        pre = call(
            functools.partial(pre_body, lanes, width), shape((2 * size, 3 * cols), F32), 2 * work
        )(*tok_list, *tok_other, first, second)
        outs = call(
            functools.partial(main_body, lanes, width),
            [shape((size, rest_width + LANES), F32), shape((size, rest_width + LANES), BF16)]
            + [shape((2 * size, 2 * cols), BF16), shape((2 * size, cols), BF16)],
            2 * work,
        )(pre, *cot_list, *cot_other, first, second, third)
        rest = outs[0] + along_core(outs[1]).astype(F32)
        owned = call(
            functools.partial(own_body, lanes, width),
            [shape((size, width), F32), shape((size, width), BF16)],
            work,
        )(outs[2], first, second)
        owned = owned[0] + along_core(owned[1]).astype(F32)
        return owned, rest, [outs[2]], [outs[3]], tok_list + tok_other, cot_list + cot_other

    near_own, near_rest, *near = experts_on(tok_near, cot_near)
    far_own, far_rest, *far = experts_on(tok_far, cot_far)
    early = 3 * width // (8 * LANES) * LANES
    if lanes == 2 and early > 0:
        near_in = along_tp(near_rest[:, early:width].astype(BF16), 1)
        lane_in = along_tp(far_rest[:, early:width].astype(BF16), 1)
        side_out = jnp.concatenate([far_rest[:, :early], far_rest[:, width:]], axis=1)
        side_in = along_side(side_out.astype(BF16)).astype(F32)
        own_in = along_side(far_own[:, :early].astype(BF16))
        last_in = along_side((far_own[:, early:] + lane_in.astype(F32)).astype(BF16))
        near_out = jnp.concatenate([near_rest[:, :early], near_rest[:, width:]], axis=1)
        next_out = near_out + side_in
        next_in = along_tp(next_out.astype(BF16), 1).astype(F32)
        tail = next_out[:, early:] + next_in[:, early:]
        left = near_own[:, :early] + own_in.astype(F32) + next_in[:, :early]
        right = near_own[:, early:] + near_in.astype(F32) + last_in.astype(F32)
        body = jnp.concatenate([left, right], axis=1)
    else:
        body = near_own + along_side(far_own.astype(BF16)).astype(F32)
        both = near_rest + along_side(far_rest.astype(BF16)).astype(F32)
        tail = both[:, rest_width:]
        for j in range(1, lanes):
            piece = jnp.concatenate(
                [both[:, (j - 1) * width : j * width], both[:, rest_width:]], axis=1
            )
            piece = along_tp(piece.astype(BF16), lanes - j).astype(F32)
            body = body + piece[:, :width]
            tail = tail + piece[:, width:]
    held = tail[:, :EPG] + tail[:, EPG : 2 * EPG]
    held = jnp.pad(held, ((0, 0), (0, LANES - EPG)))
    result = jnp.concatenate([body, held], axis=1).astype(BF16)
    sent = {k: along_groups(result[k * cap : (k + 1) * cap], k) for k in range(groups - 1, 0, -1)}
    returned = [result[:cap]] + [sent[k] for k in range(1, groups)]
    grads, scaled_hidden, toks, cots = [near[i] + far[i] for i in range(4)]
    up_work = 2 * 2 * 4 * rows * features * cols
    first_grad, second_grad = call(
        functools.partial(up_body, lanes, width, len(grads)),
        [shape((features, cols), F32)] * 2,
        up_work,
    )(*toks, *grads)
    third_grad = call(
        functools.partial(down_body, lanes, width, len(grads)),
        shape((cols, features), F32),
        up_work // 2,
    )(*cots, *scaled_hidden)
    token_grad, group_grad, expert_grad = call(
        functools.partial(final_body, groups, cap),
        [shape((count, width), F32), shape((1, count), F32), shape((picks, count), F32)],
    )(*returned, *picked, local_rows, weight_row, expert_rows)
    return (
        token_grad,
        group_grad.reshape(count),
        expert_grad.T,
        first_grad[None],
        second_grad[None],
        third_grad[None],
    )


def solution(mesh):
    in_specs = (
        P("ep", None),
        P("ep", None),
        P("ep"),
        P("ep", None),
        P("ep"),
        P("ep", None),
        P("ep", None, "tp"),
        P("ep", None, "tp"),
        P("ep", "tp", None),
    )
    out_specs = (
        P("ep", "tp"),
        P("ep"),
        P("ep", None),
        P("ep", None, "tp"),
        P("ep", None, "tp"),
        P("ep", "tp", None),
    )
    return jax.shard_map(layer, mesh=mesh, in_specs=in_specs, out_specs=out_specs, check_vma=False)
```

```python
import functools

import jax
import jax.numpy as jnp
from jax import lax
from jax.experimental import pallas as pl
from jax.experimental.pallas import tpu as pltpu
from jax.sharding import PartitionSpec as P


EPG = 4
LANES = 128
F32 = jnp.float32
BF16 = jnp.bfloat16

ROWS_COLS = (((1,), (1,)), ((), ()))
COLS_ROWS = (((1,), (0,)), ((), ()))
ROWS_ROWS = (((0,), (0,)), ((), ()))


def dot(a, b, dims):
    return lax.dot_general(a, b, dims, preferred_element_type=F32)


def call(body, outs, flops=0, space=pltpu.VMEM, scratch=()):
    def run(*args):
        return pl.pallas_call(
            body,
            out_shape=outs,
            in_specs=[pl.BlockSpec(memory_space=space)] * len(args),
            out_specs=jax.tree.map(lambda _: pl.BlockSpec(memory_space=pltpu.VMEM), outs),
            scratch_shapes=scratch,
            compiler_params=pltpu.CompilerParams(vmem_limit_bytes=40 * 2**20),
            cost_estimate=pl.CostEstimate(flops=flops, bytes_accessed=0, transcendentals=0),
        )(*args)

    return run


def route_body(groups, cap, width, *refs):
    sources = refs[:6]
    whole_out = refs[6:8]
    tok_out = refs[8 : 6 + groups]
    cot_out = refs[6 + groups : 4 + 2 * groups]
    choice_ref, local_ref, weight_ref, expert_ref, tok_ref, cot_ref, sems = refs[4 + 2 * groups :]
    count = tok_ref.shape[0]
    own = lax.axis_index("ep") // EPG
    start = pl.multiple_of(lax.axis_index("tp") * width, width)
    copies = []
    for k, (src, dst) in enumerate(
        zip(sources, (choice_ref, local_ref, weight_ref, expert_ref, tok_ref, cot_ref))
    ):
        if k >= 4:
            src = src.at[:, pl.ds(start, width)]
        copies.append(pltpu.make_async_copy(src, dst, sems.at[k]))
    for copy in copies:
        copy.start()
    for copy in copies[:4]:
        copy.wait()
    choice = choice_ref[...]
    padded = -(-groups // 8) * 8
    member = lax.broadcasted_iota(jnp.int32, (padded, count), 0) == choice
    before = (
        lax.broadcasted_iota(jnp.int32, (count, count), 0)
        < lax.broadcasted_iota(jnp.int32, (count, count), 1)
    ).astype(BF16)
    member = member.astype(F32)
    ahead = dot(member.astype(BF16), before, COLS_ROWS)
    place = jnp.sum(ahead * member, axis=0, keepdims=True).astype(jnp.int32)
    lane = lax.broadcasted_iota(jnp.int32, (LANES, count), 0)
    gates = jnp.zeros((LANES, count), F32)
    for k in range(local_ref.shape[0]):
        gate = (weight_ref[...] * expert_ref[k : k + 1, :]).astype(BF16).astype(F32)
        gates = gates + jnp.where(lane == local_ref[k : k + 1, :], gate, 0.0)
    gates = gates.astype(BF16)
    slot = lax.broadcasted_iota(jnp.int32, (cap, count), 0)
    picks = [
        ((slot == place) & (choice == (own ^ k))).astype(F32).astype(BF16)
        for k in range(groups)
    ]
    gate_rows = [dot(pick, gates, ROWS_COLS).astype(BF16) for pick in picks]
    copies[4].wait()
    for k in range(groups):
        rows = dot(picks[k], tok_ref[...], COLS_ROWS).astype(BF16)
        if k < 2:
            whole_out[k][:, :width] = rows
        else:
            tok_out[k - 2][...] = rows
    copies[5].wait()
    for k in range(groups):
        rows = dot(picks[k], cot_ref[...], COLS_ROWS).astype(BF16)
        if k < 2:
            whole_out[k][:, width : 2 * width] = rows
            whole_out[k][:, 2 * width :] = gate_rows[k]
        else:
            cot_out[k - 2][:, :width] = rows
            cot_out[k - 2][:, width:] = gate_rows[k]


def picks_body(groups, cap, parts, choice_ref, out_ref):
    choice = choice_ref[...]
    count = choice.shape[1]
    own = lax.axis_index("ep") // EPG
    padded = -(-groups // 8) * 8
    member = (lax.broadcasted_iota(jnp.int32, (padded, count), 0) == choice).astype(F32)
    before = (
        lax.broadcasted_iota(jnp.int32, (count, count), 0)
        < lax.broadcasted_iota(jnp.int32, (count, count), 1)
    ).astype(BF16)
    ahead = dot(member.astype(BF16), before, COLS_ROWS)
    place = jnp.sum(ahead * member, axis=0, keepdims=True).astype(jnp.int32)
    slot = lax.broadcasted_iota(jnp.int32, (cap, count), 0)
    for i, k in enumerate(parts):
        pick = (slot == place) & (choice == (own ^ k))
        out_ref[pl.ds(i * cap, cap), :] = pick.astype(F32).astype(BF16)


def spans_of(lanes, width):
    rank = lax.axis_index("tp")
    return [
        pl.ds(pl.multiple_of(((rank + lanes - j) % lanes) * width, width), width)
        for j in range(lanes)
    ]


def stack(parts):
    return jnp.concatenate(parts, axis=0)


def pre_body(lanes, width, *refs):
    tok = [refs[c * lanes : (c + 1) * lanes] for c in range(2)]
    gate_w, up_w, out = refs[2 * lanes :]
    cols = gate_w.shape[1]
    spans = spans_of(lanes, width)
    gate = up = 0.0
    for j in range(lanes):
        part = stack([tok[c][j][...] for c in range(2)])
        gate = gate + dot(part, gate_w[spans[j], :], COLS_ROWS)
        up = up + dot(part, up_w[spans[j], :], COLS_ROWS)
    sigma = jax.nn.sigmoid(gate)
    swish = gate * sigma
    out[:, :cols] = swish
    out[:, cols : 2 * cols] = swish * up
    out[:, 2 * cols :] = up * sigma * (1.0 + gate * (1.0 - sigma))


def main_body(lanes, width, *refs):
    pre = refs[0]
    cot = [refs[1 + c * lanes : 1 + (c + 1) * lanes] for c in range(2)]
    gate_w, up_w, down_w = refs[1 + 2 * lanes : 4 + 2 * lanes]
    keep, send, grads, scaled_hidden = refs[4 + 2 * lanes :]
    rows = keep.shape[0]
    cols = gate_w.shape[1]
    mine = lax.axis_index("ep") % EPG
    spans = spans_of(lanes, width)
    lane = lax.broadcasted_iota(jnp.int32, (2 * rows, LANES), 1)
    back = 0.0
    for j in range(lanes):
        part = stack([cot[c][j][:, :width] for c in range(2)])
        back = back + dot(part, down_w[:, spans[j]], ROWS_COLS)
    gates = stack([cot[c][0][:, width:] for c in range(2)]).astype(F32)
    gate = jnp.sum(jnp.where(lane == mine, gates, 0.0), axis=1, keepdims=True)
    hidden = pre[:, cols : 2 * cols]
    gate_part = jnp.sum(hidden * back, axis=1, keepdims=True)
    scaled = gate * back
    grad_gate = (scaled * pre[:, 2 * cols :]).astype(BF16)
    grad_up = (scaled * pre[:, :cols]).astype(BF16)
    grads[:, :cols] = grad_gate
    grads[:, cols:] = grad_up
    scaled_hidden[...] = (gate * hidden).astype(BF16)
    for j in range(1, lanes):
        total = dot(grad_gate, gate_w[spans[j], :], ROWS_COLS)
        total = total + dot(grad_up, up_w[spans[j], :], ROWS_COLS)
        keep[:, (j - 1) * width : j * width] = total[:rows]
        send[:, (j - 1) * width : j * width] = total[rows:].astype(BF16)
    high = gate_part.astype(BF16).astype(F32)
    low = gate_part - high
    tail = jnp.where(lane == mine, high, jnp.where(lane == mine + EPG, low, 0.0))
    keep[:, (lanes - 1) * width :] = tail[:rows]
    send[:, (lanes - 1) * width :] = tail[rows:].astype(BF16)


def own_body(lanes, width, grads, gate_w, up_w, keep, send):
    rows = keep.shape[0]
    cols = gate_w.shape[1]
    span = spans_of(lanes, width)[0]
    total = dot(grads[:, :cols], gate_w[span, :], ROWS_COLS)
    total = total + dot(grads[:, cols:], up_w[span, :], ROWS_COLS)
    keep[...] = total[:rows]
    send[...] = total[rows:].astype(BF16)


def up_body(lanes, width, sets, *refs):
    tok = [refs[b * lanes : (b + 1) * lanes] for b in range(2 * sets)]
    grads = stack([ref[...] for ref in refs[2 * sets * lanes : 2 * sets * lanes + sets]])
    gate_out, up_out = refs[2 * sets * lanes + sets :]
    cols = gate_out.shape[1]
    rank = lax.axis_index("tp")
    chunk = min(width, 512)
    for j in range(lanes):
        base = ((rank + lanes - j) % lanes) * width
        for s in range(0, width, chunk):
            span = pl.ds(pl.multiple_of(base + s, chunk), chunk)
            part = stack([x[j][:, s : s + chunk] for x in tok])
            total = dot(part, grads, ROWS_ROWS)
            gate_out[span, :] = total[:, :cols]
            up_out[span, :] = total[:, cols:]


def down_body(lanes, width, sets, *refs):
    cot = [refs[b * lanes : (b + 1) * lanes] for b in range(2 * sets)]
    hidden = stack([ref[...] for ref in refs[2 * sets * lanes : 2 * sets * lanes + sets]])
    down_out = refs[2 * sets * lanes + sets]
    rank = lax.axis_index("tp")
    chunk = min(width, 512)
    for j in range(lanes):
        base = ((rank + lanes - j) % lanes) * width
        for s in range(0, width, chunk):
            span = pl.ds(pl.multiple_of(base + s, chunk), chunk)
            part = stack([x[j][:, s : s + chunk] for x in cot])
            down_out[:, span] = dot(hidden, part, ROWS_ROWS)


def first_body(cap, blocks, *refs):
    back = refs[: len(blocks)]
    pick_refs = refs[len(blocks) : len(blocks) + 4]
    total_out, held_out = refs[len(blocks) + 4 :]
    count, width = total_out.shape
    total = jnp.zeros((count, width), F32)
    held = jnp.zeros((LANES, count), F32)
    for ref, k in zip(back, blocks):
        pick = pick_refs[min(k, 3)][pl.ds(max(k - 3, 0) * cap, cap), :]
        total = total + dot(pick, ref[:, :width], ROWS_ROWS)
        held = held + dot(ref[:, width:], pick, ROWS_ROWS)
    total_out[...] = total
    held_out[...] = held


def final_body(back, pick_ref, total_ref, held_ref, local_ref, weight_ref, expert_ref, *outs):
    tok_out, group_out, expert_out = outs
    count, width = tok_out.shape
    pick = pick_ref[...]
    tok_out[...] = total_ref[...] + dot(pick, back[:, :width], ROWS_ROWS)
    held = held_ref[...] + dot(back[:, width:], pick, ROWS_ROWS)
    lane = lax.broadcasted_iota(jnp.int32, (LANES, count), 0)
    group_sum = jnp.zeros((1, count), F32)
    for k in range(local_ref.shape[0]):
        grad = jnp.sum(
            jnp.where(lane == local_ref[k : k + 1, :], held, 0.0), axis=0, keepdims=True
        )
        group_sum = group_sum + expert_ref[k : k + 1, :] * grad
        expert_out[k : k + 1, :] = weight_ref[...] * grad
    group_out[...] = group_sum


def layer(
    tokens, cotangent, group_weight, expert_weight, group_choice, local_choice, w_gate, w_up, w_down
):
    count, features = tokens.shape
    picks = expert_weight.shape[1]
    experts = lax.axis_size("ep")
    lanes = lax.axis_size("tp")
    groups = experts // EPG
    width = features // lanes
    capacity = picks * (3 * count // (2 * experts))
    cap = min(count, EPG * capacity // picks)
    cap = -(-cap // 16) * 16
    rows = groups * cap
    cols = w_gate.shape[2]

    def along_groups(a, k):
        return lax.ppermute(a, "ep", [(e, e ^ (k * EPG)) for e in range(experts)])

    def along_side(a):
        return lax.ppermute(a, "ep", [(e, e ^ 2) for e in range(experts)])

    def along_core(a):
        return lax.ppermute(a, "ep", [(e, e ^ 1) for e in range(experts)])

    def along_tp(a, j):
        return lax.ppermute(a, "tp", [(r, (r + j) % lanes) for r in range(lanes)])

    core = lax.axis_index("ep") % 2

    def along_diagonal(side, lane):
        pieces = []
        for j, a in enumerate(lane, 1):
            pairs = []
            for e in range(experts):
                for r in range(lanes):
                    there = (e ^ 2) * lanes + r if e % 2 else e * lanes + (r + j) % lanes
                    pairs.append((e * lanes + r, there))
            pieces.append(lax.ppermute(jnp.where(core == 0, side, a), ("ep", "tp"), pairs))
        return pieces

    shape = jax.ShapeDtypeStruct
    choice_row = group_choice.reshape(1, count)
    weight_row = group_weight.reshape(1, count)
    local_rows = local_choice.T
    expert_rows = expert_weight.T
    routed = call(
        functools.partial(route_body, groups, cap, width),
        [shape((cap, 2 * width + LANES), BF16)] * 2
        + [shape((cap, width), BF16)] * (groups - 2)
        + [shape((cap, width + LANES), BF16)] * (groups - 2),
        space=pltpu.HBM,
        scratch=[
            pltpu.VMEM((1, count), jnp.int32),
            pltpu.VMEM((picks, count), jnp.int32),
            pltpu.VMEM((1, count), F32),
            pltpu.VMEM((picks, count), F32),
            pltpu.VMEM((count, width), BF16),
            pltpu.VMEM((count, width), BF16),
            pltpu.SemaphoreType.DMA((6,)),
        ],
    )(
        *(
            pltpu.with_memory_space_constraint(a, pltpu.HBM)
            for a in (choice_row, local_rows, weight_row, expert_rows, tokens, cotangent)
        )
    )
    parts = [[0], [1], [2], list(range(3, groups))]
    picked = [
        call(
            functools.partial(picks_body, groups, cap, part),
            shape((len(part) * cap, count), BF16),
            10**6,
        )(choice_row)
        for part in parts
    ]
    others = range(groups - 1, 1, -1)
    next_sent = along_groups(routed[1], 1)
    tok_sent = {k: along_groups(routed[k], k) for k in others}

    def join(head, rest):
        return jnp.concatenate([head, rest], axis=0)

    def along_mixed(a, flip):
        pairs = []
        for e in range(experts):
            for r in range(lanes):
                across = (e + flip) % 2
                there = (e ^ 2) * lanes + r if across else e * lanes + (r + 1) % lanes
                pairs.append((e * lanes + r, there))
        return lax.ppermute(a, ("ep", "tp"), pairs)

    next_side = along_side(next_sent)
    next_lane = [along_tp(next_sent[:, : 2 * width], j) for j in range(1, lanes)]
    if lanes == 2:
        step = along_mixed(routed[0], 1)
        steps = along_mixed(join(routed[0], step), 0)
        own_side = jnp.where(core == 0, step, steps[:cap])
        own_lane = [jnp.where(core == 0, steps[:cap], step)[:, : 2 * width]]
        own_both = [steps[cap:, : 2 * width]]
        next_both = along_diagonal(next_side[:, : 2 * width], next_lane)
    else:
        own_side = along_side(routed[0])
        own_lane = [along_tp(routed[0][:, : 2 * width], j) for j in range(1, lanes)]
        own_both = along_diagonal(own_side[:, : 2 * width], own_lane)
        next_both = along_diagonal(next_side[:, : 2 * width], next_lane)
    own = join(routed[0], next_sent)
    own_side = join(own_side, next_side)
    own_lane = [join(a, b) for a, b in zip(own_lane, next_lane)]
    own_both = [join(a, b) for a, b in zip(own_both, next_both)]
    cot_sent = {k: along_groups(routed[groups - 2 + k], k) for k in range(2, groups)}
    tok = jnp.concatenate([tok_sent[k] for k in range(2, groups)], axis=0)
    cot = jnp.concatenate([cot_sent[k] for k in range(2, groups)], axis=0)
    cot_bare = jnp.concatenate([cot_sent[k][:, :width] for k in range(2, groups)], axis=0)
    tok_side = along_side(tok)
    tok_lane = [along_tp(tok, j) for j in range(1, lanes)]
    cot_side = along_side(cot)
    cot_lane = [along_tp(cot_bare, j) for j in range(1, lanes)]
    tok_both = along_diagonal(tok_side, tok_lane)
    cot_both = along_diagonal(cot_side[:, :width], cot_lane)

    tok_near = [join(own[:, :width], tok)]
    tok_near += [join(a[:, :width], b) for a, b in zip(own_lane, tok_lane)]
    cot_near = [join(own[:, width:], cot)]
    cot_near += [join(a[:, width:], b) for a, b in zip(own_lane, cot_lane)]
    tok_far = [join(own_side[:, :width], tok_side)]
    tok_far += [join(a[:, :width], b) for a, b in zip(own_both, tok_both)]
    cot_far = [join(own_side[:, width:], cot_side)]
    cot_far += [join(a[:, width:], b) for a, b in zip(own_both, cot_both)]
    first, second, third = w_gate[0], w_up[0], w_down[0]
    rest_width = features - width

    def experts_on(tok_list, cot_list):
        size = tok_list[0].shape[0]
        work = 2 * 2 * size * features * cols
        tok_other = [along_core(tok_list[0])]
        cot_other = [along_core(cot_list[0])]
        tok_other += [along_core(a) for a in tok_list[1:]]
        cot_other += [along_core(a) for a in cot_list[1:]]
        pre = call(
            functools.partial(pre_body, lanes, width), shape((2 * size, 3 * cols), F32), 2 * work
        )(*tok_list, *tok_other, first, second)
        outs = call(
            functools.partial(main_body, lanes, width),
            [shape((size, rest_width + LANES), F32), shape((size, rest_width + LANES), BF16)]
            + [shape((2 * size, 2 * cols), BF16), shape((2 * size, cols), BF16)],
            2 * work,
        )(pre, *cot_list, *cot_other, first, second, third)
        rest = outs[0] + along_core(outs[1]).astype(F32)
        owned = call(
            functools.partial(own_body, lanes, width),
            [shape((size, width), F32), shape((size, width), BF16)],
            work,
        )(outs[2], first, second)
        owned = owned[0] + along_core(owned[1]).astype(F32)
        return owned, rest, [outs[2]], [outs[3]], tok_list + tok_other, cot_list + cot_other

    near_own, near_rest, *near = experts_on(tok_near, cot_near)
    far_own, far_rest, *far = experts_on(tok_far, cot_far)
    early = 3 * width // (8 * LANES) * LANES
    if lanes == 2 and early > 0:
        near_in = along_tp(near_rest[:, early:width].astype(BF16), 1)
        lane_in = along_tp(far_rest[:, early:width].astype(BF16), 1)
        side_out = jnp.concatenate([far_rest[:, :early], far_rest[:, width:]], axis=1)
        side_in = along_side(side_out.astype(BF16)).astype(F32)
        own_in = along_side(far_own[:, :early].astype(BF16))
        last_in = along_side((far_own[:, early:] + lane_in.astype(F32)).astype(BF16))
        near_out = jnp.concatenate([near_rest[:, :early], near_rest[:, width:]], axis=1)
        next_out = near_out + side_in
        next_in = along_tp(next_out.astype(BF16), 1).astype(F32)
        tail = next_out[:, early:] + next_in[:, early:]
        left = near_own[:, :early] + own_in.astype(F32) + next_in[:, :early]
        right = near_own[:, early:] + near_in.astype(F32) + last_in.astype(F32)
        body = jnp.concatenate([left, right], axis=1)
    else:
        body = near_own + along_side(far_own.astype(BF16)).astype(F32)
        both = near_rest + along_side(far_rest.astype(BF16)).astype(F32)
        tail = both[:, rest_width:]
        for j in range(1, lanes):
            piece = jnp.concatenate(
                [both[:, (j - 1) * width : j * width], both[:, rest_width:]], axis=1
            )
            piece = along_tp(piece.astype(BF16), lanes - j).astype(F32)
            body = body + piece[:, :width]
            tail = tail + piece[:, width:]
    held = tail[:, :EPG] + tail[:, EPG : 2 * EPG]
    held = jnp.pad(held, ((0, 0), (0, LANES - EPG)))
    result = jnp.concatenate([body, held], axis=1).astype(BF16)
    blocks = [k for k in range(groups) if k != 2]
    sent = {k: along_groups(result[k * cap : (k + 1) * cap], k) for k in blocks[:0:-1]}
    mid = along_groups(result[2 * cap : 3 * cap], 2)
    returned = [result[:cap]] + [sent[k] for k in blocks[1:]]
    part = call(
        functools.partial(first_body, cap, blocks),
        [shape((count, width), F32), shape((LANES, count), F32)],
        10**6,
    )(*returned, *picked)
    grads, scaled_hidden, toks, cots = [near[i] + far[i] for i in range(4)]
    up_work = 2 * 2 * 4 * rows * features * cols
    first_grad, second_grad = call(
        functools.partial(up_body, lanes, width, len(grads)),
        [shape((features, cols), F32)] * 2,
        up_work,
    )(*toks, *grads)
    third_grad = call(
        functools.partial(down_body, lanes, width, len(grads)),
        shape((cols, features), F32),
        up_work // 2,
    )(*cots, *scaled_hidden)
    token_grad, group_grad, expert_grad = call(
        final_body, [shape((count, width), F32), shape((1, count), F32), shape((picks, count), F32)]
    )(mid, picked[2], *part, local_rows, weight_row, expert_rows)
    return (
        token_grad,
        group_grad.reshape(count),
        expert_grad.T,
        first_grad[None],
        second_grad[None],
        third_grad[None],
    )


def solution(mesh):
    in_specs = (
        P("ep", None),
        P("ep", None),
        P("ep"),
        P("ep", None),
        P("ep"),
        P("ep", None),
        P("ep", None, "tp"),
        P("ep", None, "tp"),
        P("ep", "tp", None),
    )
    out_specs = (
        P("ep", "tp"),
        P("ep"),
        P("ep", None),
        P("ep", None, "tp"),
        P("ep", None, "tp"),
        P("ep", "tp", None),
    )
    return jax.shard_map(layer, mesh=mesh, in_specs=in_specs, out_specs=out_specs, check_vma=False)
```
